128 devices in a mesh: sp: 32 (over z, y, core), tp: 4 (over x).
Axes of the slice: x: 4, y: 4, z: 4, core: 2. Of those that a mesh axis runs over, the one named last changes fastest.
Arguments:
- tokens: bfloat16 [32768, 2048], P('sp', 'tp'), may hold values from -6 to 6
- mix_gain: float32 [2048], replicated, may hold values from 0.1 to 1.9
- query_weight: bfloat16 [2048, 1024], P('sp', 'tp'), may hold values from -0.125 to 0.125
- key_weight: bfloat16 [2048, 256], P('sp', 'tp'), may hold values from -0.125 to 0.125
- value_weight: bfloat16 [2048, 256], P('sp', 'tp'), may hold values from -0.125 to 0.125
- conv_value_weight: bfloat16 [2048, 1024], P('sp', 'tp'), may hold values from -0.125 to 0.125
- conv_gate_weight: bfloat16 [2048, 1024], P('sp', 'tp'), may hold values from -0.125 to 0.125
- query_gain: float32 [64], replicated, may hold values from 0.1 to 1.9
- key_gain: float32 [64], replicated, may hold values from 0.1 to 1.9
- sink_logit: float32 [16], P('tp'), may hold values from 3 to 7
- conv_taps: float32 [31, 1024], P(None, 'tp'), may hold values from -1 to 1
- conv_gain: float32 [1024], P('tp'), may hold values from 0.1 to 1.9
- attn_proj: bfloat16 [1024, 2048], P('tp', 'sp'), may hold values from -1.5 to 1.5
- conv_proj: bfloat16 [1024, 2048], P('tp', 'sp'), may hold values from -0.1875 to 0.1875
Outputs:
- mixed: bfloat16 [32768, 2048], P(('sp', 'tp'))
The draws below stay inside these ranges and needn't reach their ends.
All inputs are finite; a program needn't handle non-finite values.
Results may differ from the reference program's by a relative error of at most 0.0079.
Values may be sent and summed in bfloat16 or wider, within the bound.
A program may use at most 128 MiB of HBM per device.

```python
import jax
import jax.numpy as jnp
from jax import lax

MODEL_DIM = 2048
QUERY_HEADS = 16
KEY_HEADS = 4
HEAD_DIM = 64
CHANNELS = 1024
KERNEL = 31
WINDOW = 128
LOCAL_TOKENS = 1024
TOKENS = 32768
CONV_REACH = 15


def levels(key, shape, shards, low, high):
    level = 1.0
    for dim, shards_of in shards:
        heights = jax.random.uniform(jax.random.fold_in(jax.random.fold_in(key, 6), dim), (shards_of,), jnp.float32, low / len(shards), high / len(shards))
        level = level * jnp.repeat(jnp.exp(heights), shape[dim] // shards_of).reshape((-1,) + (1,) * (len(shape) - 1 - dim))
    return level


def scatter_about(rng, shape, deviation, most, cuts=(), kind=jnp.bfloat16):
    drawn = jax.random.normal(rng, shape, jnp.float32) * deviation
    if len(cuts) > 0:
        drawn = levels(rng, shape, cuts, -0.22, 0.18) * drawn
    return jnp.clip(drawn, min=-most, max=most).astype(kind)


def setup_inputs(seed: int = 0) -> dict:
    seeds = jax.random.split(jax.random.key(seed), 15)
    return {
        "tokens": scatter_about(seeds[0], (TOKENS, MODEL_DIM), 1.0, 6.0, ((0, 32), (1, 4))),
        "mix_gain": jnp.clip(1.0 + 0.18 * jax.random.normal(seeds[1], (MODEL_DIM,), jnp.float32), 0.1, 1.9),
        "query_weight": scatter_about(seeds[2], (MODEL_DIM, QUERY_HEADS * HEAD_DIM), MODEL_DIM ** -0.5, 0.125, ((0, 32), (1, 4))),
        "key_weight": scatter_about(seeds[3], (MODEL_DIM, KEY_HEADS * HEAD_DIM), MODEL_DIM ** -0.5, 0.125, ((0, 32), (1, 4))),
        "value_weight": scatter_about(seeds[4], (MODEL_DIM, KEY_HEADS * HEAD_DIM), MODEL_DIM ** -0.5, 0.125, ((0, 32), (1, 4))),
        "conv_value_weight": scatter_about(seeds[5], (MODEL_DIM, CHANNELS), MODEL_DIM ** -0.5, 0.125, ((0, 32), (1, 4))),
        "conv_gate_weight": scatter_about(seeds[6], (MODEL_DIM, CHANNELS), MODEL_DIM ** -0.5, 0.125, ((0, 32), (1, 4))),
        "query_gain": jnp.clip(1.0 + 0.18 * jax.random.normal(seeds[7], (HEAD_DIM,), jnp.float32), 0.1, 1.9),
        "key_gain": jnp.clip(1.0 + 0.18 * jax.random.normal(seeds[8], (HEAD_DIM,), jnp.float32), 0.1, 1.9),
        "sink_logit": jnp.clip(3.0 + 4.0 * jax.random.uniform(seeds[9], (QUERY_HEADS,), jnp.float32) ** levels(seeds[9], (QUERY_HEADS,), ((0, 4),), -0.2, 0.2), 3.0, 7.0),
        "conv_taps": scatter_about(seeds[10], (KERNEL, CHANNELS), KERNEL ** -0.5, 1.0, ((1, 4),), jnp.float32),
        "conv_gain": jnp.clip(1.0 + 0.18 * jax.random.normal(seeds[11], (CHANNELS,), jnp.float32), 0.1, 1.9),
        "attn_proj": scatter_about(seeds[12], (QUERY_HEADS * HEAD_DIM, MODEL_DIM), (QUERY_HEADS * HEAD_DIM // 64) ** -0.5, 1.5, ((0, 4), (1, 32))),
        "conv_proj": scatter_about(seeds[13], (CHANNELS, MODEL_DIM), CHANNELS ** -0.5, 0.1875, ((0, 4), (1, 32))),
    }


EPSILON = 0.1

def unit_rows(values, gain):
    return values * lax.rsqrt(lax.optimization_barrier(jnp.mean(values * values, axis=-1, keepdims=True)) + EPSILON) * gain

def attend(queries, keys, values, sinks, offset, total):
    scale = queries.shape[-1] ** (-0.5)
    scores = jnp.einsum('qkgd,skd->kgqs', queries.astype(jnp.float32), keys.astype(jnp.float32)) * scale
    query_pos = offset + jnp.arange(queries.shape[0], dtype=jnp.int32)
    key_pos = offset - WINDOW + jnp.arange(keys.shape[0], dtype=jnp.int32)
    allowed = (jnp.abs(key_pos[None, :] - query_pos[:, None]) <= WINDOW) & (key_pos[None, :] >= 0) & (key_pos[None, :] < total)
    weights = jnp.where(allowed, jnp.exp(scores), 0.0)
    denominator = lax.optimization_barrier(jnp.sum(weights, axis=-1, keepdims=True)) + jnp.exp(sinks).reshape(keys.shape[1], -1, 1, 1)
    shares = (weights / denominator).astype(jnp.bfloat16)
    result = jnp.einsum('kgqs,skd->qkgd', shares.astype(jnp.float32), values.astype(jnp.float32))
    return result.reshape(queries.shape[0], -1).astype(jnp.bfloat16)

def depthwise(extended, kernel_taps, count):
    result = jnp.zeros((count, kernel_taps.shape[1]), jnp.float32)
    for offset in range(kernel_taps.shape[0]):
        result = result + kernel_taps[offset] * extended[offset:offset + count].astype(jnp.float32)
    return result

def reference(tokens, mix_gain, query_weight, key_weight, value_weight, conv_value_weight, conv_gate_weight, query_gain, key_gain, sink_logit, conv_taps, conv_gain, attn_proj, conv_proj):
    total = tokens.shape[0]
    normed = unit_rows(tokens.astype(jnp.float32), mix_gain).astype(jnp.bfloat16)
    query = jnp.dot(normed, query_weight, preferred_element_type=jnp.float32)
    key_part = jnp.dot(normed, key_weight, preferred_element_type=jnp.float32)
    value_part = jnp.dot(normed, value_weight, preferred_element_type=jnp.float32)
    conv_value = jnp.dot(normed, conv_value_weight, preferred_element_type=jnp.float32)
    conv_gate = jnp.dot(normed, conv_gate_weight, preferred_element_type=jnp.float32)
    group = QUERY_HEADS // KEY_HEADS
    queries = unit_rows(query.reshape(total, KEY_HEADS, group, HEAD_DIM), query_gain).astype(jnp.bfloat16)
    keys = unit_rows(key_part.reshape(total, KEY_HEADS, HEAD_DIM), key_gain).astype(jnp.bfloat16)
    values = value_part.reshape(total, KEY_HEADS, HEAD_DIM).astype(jnp.bfloat16)
    padded_keys = jnp.pad(keys, ((WINDOW, WINDOW), (0, 0), (0, 0)))
    padded_values = jnp.pad(values, ((WINDOW, WINDOW), (0, 0), (0, 0)))

    def one_block(index):
        begin = (index * LOCAL_TOKENS).astype(jnp.int32)
        block_queries = lax.dynamic_slice_in_dim(queries, begin, LOCAL_TOKENS, 0)
        block_keys = lax.dynamic_slice_in_dim(padded_keys, begin, LOCAL_TOKENS + 2 * WINDOW, 0)
        block_values = lax.dynamic_slice_in_dim(padded_values, begin, LOCAL_TOKENS + 2 * WINDOW, 0)
        return attend(block_queries, block_keys, block_values, sink_logit, begin, total)
    attended = lax.map(one_block, jnp.arange(total // LOCAL_TOKENS, dtype=jnp.int32)).reshape(total, -1)
    gated = (conv_value * jax.nn.sigmoid(conv_gate)).astype(jnp.bfloat16)
    extended = jnp.pad(gated, ((CONV_REACH, CONV_REACH), (0, 0)))
    convolved = depthwise(extended, conv_taps, total)
    center = lax.optimization_barrier(jnp.mean(convolved, axis=1, keepdims=True))
    centered = convolved - center
    spread = lax.optimization_barrier(jnp.mean(centered * centered, axis=1, keepdims=True))
    featured = jax.nn.silu(centered * lax.rsqrt(spread + EPSILON) * conv_gain).astype(jnp.bfloat16)
    summed = jnp.dot(attended, attn_proj, preferred_element_type=jnp.float32) + jnp.dot(featured, conv_proj, preferred_element_type=jnp.float32)
    return summed.astype(jnp.bfloat16)
```

```python
import jax
import jax.numpy as jnp
from jax import lax
from jax.sharding import PartitionSpec as P

WINDOW = 128
EPSILON = 0.1
BOTH = ("sp", "tp")


def unit_rows(values, gain):
    return values * lax.rsqrt(jnp.mean(values * values, axis=-1, keepdims=True) + EPSILON) * gain


def halo(value, width):
    size = lax.axis_size("sp") * lax.axis_size("tp")
    up = [(i, i + 1) for i in range(size - 1)]
    down = [(i + 1, i) for i in range(size - 1)]
    before = lax.ppermute(value[-width:], BOTH, up)
    after = lax.ppermute(value[:width], BOTH, down)
    return jnp.concatenate([before, value, after], axis=0)


def attend(queries, keys, values, sinks, offset, total):
    scale = queries.shape[-1] ** (-0.5)
    scores = jnp.einsum("qkgd,skd->kgqs", queries, keys, preferred_element_type=jnp.float32) * scale
    query_pos = offset + jnp.arange(queries.shape[0], dtype=jnp.int32)
    key_pos = offset - WINDOW + jnp.arange(keys.shape[0], dtype=jnp.int32)
    allowed = (
        (jnp.abs(key_pos[None, :] - query_pos[:, None]) <= WINDOW)
        & (key_pos[None, :] >= 0)
        & (key_pos[None, :] < total)
    )
    weights = jnp.where(allowed, jnp.exp(scores), 0.0)
    denominator = jnp.sum(weights, axis=-1, keepdims=True) + jnp.exp(sinks).reshape(
        keys.shape[1], -1, 1, 1
    )
    shares = (weights / denominator).astype(jnp.bfloat16)
    result = jnp.einsum("kgqs,skd->qkgd", shares, values, preferred_element_type=jnp.float32)
    return result.reshape(queries.shape[0], -1).astype(jnp.bfloat16)


def depthwise(extended, kernel_taps, count):
    result = jnp.zeros((count, kernel_taps.shape[1]), jnp.float32)
    for offset in range(kernel_taps.shape[0]):
        result = result + kernel_taps[offset] * extended[offset : offset + count]
    return result


def on_device(tokens, mix_gain, wq, wk, wv, wcv, wcg, query_gain, key_gain, sinks, taps, conv_gain, attn_proj, conv_proj):
    tps = lax.axis_size("tp")
    count = tokens.shape[0] // tps
    w_in = lax.all_gather(jnp.concatenate([wq, wk, wv, wcv, wcg], axis=1), ("tp", "sp"), axis=0, tiled=True)
    w_in = w_in.reshape(tps, -1, w_in.shape[1])
    w_out = lax.all_gather(jnp.concatenate([attn_proj.T, conv_proj.T], axis=1), ("tp", "sp"), axis=0, tiled=True)
    w_out = w_out.reshape(tps, -1, w_out.shape[1])
    taps = jnp.moveaxis(lax.all_gather(taps, "tp"), 0, 1).reshape(taps.shape[0], -1)
    conv_gain = lax.all_gather(conv_gain, "tp", tiled=True)
    sinks = lax.all_gather(sinks, "tp", tiled=True)
    mine = lax.all_to_all(tokens.reshape(tps, count, -1), "tp", 0, 0, tiled=True)
    whole = jnp.moveaxis(mine, 0, 1).reshape(count, -1)
    normed = unit_rows(whole.astype(jnp.float32), mix_gain).astype(jnp.bfloat16)
    out = jnp.einsum("tk,pkc->tpc", normed, w_in, preferred_element_type=jnp.float32)
    head = query_gain.shape[0]
    widths = [wq.shape[1], wk.shape[1], wv.shape[1], wcv.shape[1]]
    ends = [sum(widths[: k + 1]) for k in range(4)]
    query, key_part, value_part, conv_value, conv_gate = jnp.split(out, ends, axis=2)
    kv = tps * key_part.shape[2] // head
    group = query.shape[2] * tps // head // kv
    queries = unit_rows(query.reshape(count, kv, group, head), query_gain).astype(jnp.bfloat16)
    keys = unit_rows(key_part.reshape(count, kv, head), key_gain).astype(jnp.bfloat16).reshape(count, -1)
    values = value_part.reshape(count, -1).astype(jnp.bfloat16)
    gated = (conv_value * jax.nn.sigmoid(conv_gate)).astype(jnp.bfloat16).reshape(count, -1)
    reach = (taps.shape[0] - 1) // 2
    ext_kv = halo(jnp.concatenate([keys, values], axis=1), WINDOW)
    ext_conv = halo(gated, 16)[16 - reach : 16 + count + reach]
    index = lax.axis_index("sp") * tps + lax.axis_index("tp")
    total = count * tps * lax.axis_size("sp")
    half = keys.shape[1]
    span = ext_kv.shape[0]
    attended = attend(
        queries, ext_kv[:, :half].reshape(span, kv, head), ext_kv[:, half:].reshape(span, kv, head),
        sinks, index * count, total,
    )
    convolved = depthwise(ext_conv, taps, count)
    center = jnp.mean(convolved, axis=1, keepdims=True)
    centered = convolved - center
    spread = jnp.mean(centered * centered, axis=1, keepdims=True)
    featured = jax.nn.silu(centered * lax.rsqrt(spread + EPSILON) * conv_gain).astype(jnp.bfloat16)
    feats = jnp.concatenate([attended.reshape(count, tps, -1), featured.reshape(count, tps, -1)], axis=2)
    mixed = jnp.einsum("tpk,pok->to", feats, w_out, preferred_element_type=jnp.float32)
    return mixed.astype(jnp.bfloat16)


def solution(mesh):
    placed = (
        P("sp", "tp"), P(), P("sp", "tp"), P("sp", "tp"), P("sp", "tp"), P("sp", "tp"), P("sp", "tp"),
        P(), P(), P("tp"), P(None, "tp"), P("tp"), P("tp", "sp"), P("tp", "sp"),
    )
    return jax.shard_map(
        on_device, mesh=mesh, in_specs=placed, out_specs=P(("sp", "tp"), None), check_vma=False
    )
```

```python
import jax
import jax.numpy as jnp
from jax import lax
from jax.experimental import pallas as pl
from jax.experimental.pallas import tpu as pltpu
from jax.sharding import PartitionSpec as P

MESH = pl.DeviceIdType.MESH
EPSILON = 0.1
BF = jnp.bfloat16
F32 = jnp.float32

CV, CG, KV, Q = (0, 256), (256, 512), (512, 640), (640, 896)
STAGES = (
    ("w", 0, 640, ((0, 48, 32), (48, 32, 16), (80, 48, 32))),
    ("w", 640, 256, ((0, 32, 16), (32, 48, 32), (80, 48, 32))),
    ("p", 0, 128, ((0, 176, 96), (176, 160, 80), (336, 176, 96))),
)
ORDERS = ("xyz", "yzx", "zxy")


def kernel(
    tokens, mix_gain, wq, wk, wv, wcv, wcg, query_gain, key_gain, sink_row, taps, conv_gain, attn_proj, conv_proj,
    out,
    w, p, mine_w, mine_p, peer_p, small, x_buf, normed, qn, kve, ge, conv, stat_own, stat_peer, feats,
    part_own, part_send, part_recv,
    ag_send, ag_recv, d2d_send, d2d_recv, tok_send, tok_recv, fwd_send, fwd_recv, loc_sem, sm_send, sm_recv,
    halo_send, halo_recv, stat_send, stat_recv, out_send, out_recv,
):
    sp, x = lax.axis_index("sp"), lax.axis_index("tp")
    k = lax.rem(sp, 2)
    q = sp // 2
    y, z = lax.rem(q, 4), q // 4
    pos = lax.rem(x + 4 - 2 * k, 4)
    xi0 = lax.rem(x, 2)
    is_source = pos < 2
    bufs = {"w": w, "p": p}

    def dev(xx, yy, zz, kk):
        return (zz * 8 + yy * 2 + kk, xx)

    def up(v, n=1):
        return lax.rem(v + n, 4)

    peer = dev(x, y, z, 1 - k)
    sends = []

    def copy(src, dst, ssem, rsem, device):
        return pltpu.make_async_remote_copy(
            src_ref=src, dst_ref=dst, send_sem=ssem, recv_sem=rsem, device_id=device, device_id_type=MESH
        )

    def send(src, dst, ssem, rsem, device, cond=None):
        def go():
            copy(src, dst, ssem, rsem, device).start()

        if cond is None:
            go()
        else:
            pl.when(cond)(go)
        sends.append((src, dst, ssem, rsem, device, cond))

    def recv(dst, ssem, rsem, cond=None):
        def go():
            copy(dst, dst, ssem, rsem, peer).wait_recv()

        if cond is None:
            go()
        else:
            pl.when(cond)(go)

    def ref_of(stage, color, phase, where, half):
        name, c0, cn, rows = STAGES[stage]
        buf = bufs[name]
        r0, rn, rh = rows[color]
        cols = pl.ds(c0, cn)
        rr = pl.ds(r0, rn)
        parts = {None: rr, 0: pl.ds(r0, rh), 1: pl.ds(r0 + rh, rn - rh)}
        two = {None: slice(None), 0: pl.ds(0, 2), 1: pl.ds(2, 2)}
        one = {None: slice(None), 0: pl.ds(0, 1), 1: pl.ds(1, 1)}
        axis = ORDERS[color][phase]
        if phase == 0:
            if axis == "x":
                return buf.at[where, z, y, parts[half], cols]
            if axis == "y":
                return buf.at[xi0, z, where, parts[half], cols]
            return buf.at[xi0, where, y, parts[half], cols]
        if color == 0:
            if axis == "y":
                return buf.at[one[half], z, where, rr, cols]
            return buf.at[one[half], where, :, rr, cols]
        if color == 1:
            if axis == "z":
                return buf.at[xi0, where, two[half], rr, cols]
            return buf.at[where, two[half], :, rr, cols]
        if axis == "x":
            return buf.at[where, two[half], y, rr, cols]
        return buf.at[one[half], :, where, rr, cols]

    def context(stage, color, phase):
        axis = ORDERS[color][phase]
        base = ((stage * 3 + color) * 3 + phase) * 4
        ss = [ag_send.at[base + i] for i in range(4)]
        rs = [ag_recv.at[base + i] for i in range(4)]
        only_sources = is_source if ORDERS[color].index("x") > phase else None
        return axis, ss, rs, only_sources

    def ring(axis):
        if axis == "y":
            return y, dev(x, up(y), z, k), dev(x, up(y, 3), z, k)
        return z, dev(x, y, up(z), k), dev(x, y, up(z, 3), k)

    def start1(stage, color, phase):
        axis, ss, rs, cond = context(stage, color, phase)
        if axis == "x":
            r = ref_of(stage, color, phase, xi0, None)
            send(r, r, ss[0], rs[0], dev(up(x), y, z, k), is_source)
            send(r, r, ss[1], rs[0], dev(up(x, 3), y, z, k), is_source)
        else:
            at, right, left = ring(axis)
            r = ref_of(stage, color, phase, at, None)
            send(r, r, ss[0], rs[0], right, cond)
            send(r, r, ss[1], rs[1], left, cond)

    def turn(stage, color, phase):
        axis, ss, rs, cond = context(stage, color, phase)
        if axis == "x":
            other = 1 - xi0
            recv(ref_of(stage, color, phase, other, None), ss[0], rs[0])
            h0 = ref_of(stage, color, phase, other, 0)
            h1 = ref_of(stage, color, phase, other, 1)
            to_low = dev(jnp.where(pos == 0, up(x, 3), up(x)), y, z, k)
            to_high = dev(jnp.where(pos == 2, up(x), up(x, 3)), y, z, k)
            send(h0, h0, ss[2], rs[2], to_low, pos < 2)
            send(h1, h1, ss[3], rs[3], to_high, pos >= 2)
        else:
            at, right, left = ring(axis)
            recv(ref_of(stage, color, phase, up(at, 3), None), ss[0], rs[0], cond)
            h0 = ref_of(stage, color, phase, up(at, 3), 0)
            send(h0, h0, ss[2], rs[2], right, cond)
            recv(ref_of(stage, color, phase, up(at), None), ss[1], rs[1], cond)
            h1 = ref_of(stage, color, phase, up(at), 1)
            send(h1, h1, ss[3], rs[3], left, cond)

    def finish(stage, color, phase):
        axis, ss, rs, cond = context(stage, color, phase)
        if axis == "x":
            recv(ref_of(stage, color, phase, xi0, 0), ss[2], rs[2], pos >= 2)
            recv(ref_of(stage, color, phase, xi0, 1), ss[3], rs[3], pos >= 2)
        else:
            at, _, _ = ring(axis)
            recv(ref_of(stage, color, phase, up(at, 2), 0), ss[2], rs[2], cond)
            recv(ref_of(stage, color, phase, up(at, 2), 1), ss[3], rs[3], cond)

    def all_colors(step, stage, phase):
        for color in range(3):
            step(stage, color, phase)

    own_rows = pl.ds(pl.multiple_of(k * 64, 64), 64)
    shard = jnp.concatenate([wcv[...], wcg[...], wk[...], wv[...], wq[...]], axis=1)

    @pl.when(is_source)
    def _():
        w[xi0, z, y, own_rows, :] = shard

    @pl.when(jnp.logical_not(is_source))
    def _():
        mine_w[...] = shard

    mine_p[...] = jnp.concatenate([attn_proj[...], conv_proj[...]], axis=1)
    small[xi0, 0:31, :] = taps[...]
    small[xi0, 31:32, :] = conv_gain[...]
    small[xi0, 32:33, :] = sink_row[...]

    barrier = pltpu.get_barrier_semaphore()
    y_up, z_up = up(y), up(z)
    q_next, q_last = lax.rem(q + 1, 16), lax.rem(q + 15, 16)
    partners = [
        peer, dev(up(x), y, z, k), dev(up(x, 2), y, z, k), dev(up(x, 3), y, z, k),
        dev(x, y_up, z, k), dev(x, up(y, 3), z, k), dev(x, y, z_up, k), dev(x, y, up(z, 3), k),
        (q_next * 2 + k, up(x)), (q_last * 2 + k, up(x, 3)),
    ]
    for partner in partners:
        pl.semaphore_signal(barrier, inc=1, device_id=partner, device_id_type=MESH)
    pl.semaphore_wait(barrier, len(partners))

    not_source = jnp.logical_not(is_source)
    slot = w.at[xi0, z, y, own_rows, :]
    send(mine_w, slot, d2d_send.at[0], d2d_recv.at[0], peer, not_source)
    send(mine_p, peer_p, d2d_send.at[1], d2d_recv.at[1], peer)
    peer_rows = pl.ds(pl.multiple_of((1 - k) * 64, 64), 64)
    recv(w.at[xi0, z, y, peer_rows, :], d2d_send.at[0], d2d_recv.at[0], is_source)
    all_colors(start1, 0, 0)

    for d in (1, 3, 2):
        to = up(x, d)
        rows = pl.ds(pl.multiple_of(to * 256, 256), 256)
        send(tokens.at[rows, :], x_buf.at[k, x], tok_send.at[d], tok_recv.at[d], dev(to, y, z, k))
    rows = pl.ds(pl.multiple_of(x * 256, 256), 256)
    local = pltpu.make_async_copy(tokens.at[rows, :], x_buf.at[k, x], loc_sem)
    local.start()
    send(tokens.at[rows, :], x_buf.at[k, x], fwd_send.at[0], fwd_recv.at[0], peer)
    mine_small = small.at[xi0]
    for d in (1, 2, 3):
        send(mine_small, mine_small, sm_send.at[d], sm_recv.at[xi0], dev(up(x, d), y, z, k), is_source)

    all_colors(turn, 0, 0)
    all_colors(start1, 1, 0)
    all_colors(finish, 0, 0)
    all_colors(start1, 0, 1)

    recv(peer_p, d2d_send.at[1], d2d_recv.at[1])

    @pl.when(is_source)
    def _():
        a, b = mine_p[...], peer_p[...]
        low = jnp.where(k == 0, a, b)
        high = jnp.where(k == 0, b, a)
        p[xi0, z, y, 0:256, :] = jnp.concatenate([low[:, :64], high[:, :64]], axis=1)
        p[xi0, z, y, 256:512, :] = jnp.concatenate([low[:, 64:], high[:, 64:]], axis=1)

    all_colors(turn, 1, 0)
    all_colors(turn, 0, 1)
    all_colors(finish, 1, 0)
    all_colors(finish, 0, 1)
    all_colors(start1, 0, 2)
    all_colors(start1, 1, 1)
    all_colors(start1, 2, 0)

    for d in (1, 3, 2):
        origin = up(x, 4 - d)
        recv(x_buf.at[k, origin], tok_send.at[d], tok_recv.at[d])
        send(x_buf.at[k, origin], x_buf.at[k, origin], fwd_send.at[d], fwd_recv.at[d], peer)

    all_colors(turn, 2, 0)
    all_colors(turn, 1, 1)
    all_colors(finish, 2, 0)
    all_colors(finish, 1, 1)

    local.wait()
    recv(x_buf.at[1 - k, x], fwd_send.at[0], fwd_recv.at[0])
    for d in (1, 3, 2):
        recv(x_buf.at[1 - k, up(x, 4 - d)], fwd_send.at[d], fwd_recv.at[d])

    def norm_rows(i, _):
        s, r = i // 8, lax.rem(i, 8)
        rows = pl.ds(pl.multiple_of(r * 32, 32), 32)
        parts = [x_buf[s, f, rows, :].astype(F32) for f in range(4)]
        square = sum(jnp.sum(v * v, axis=-1, keepdims=True) for v in parts)
        scale = lax.rsqrt(square * (1.0 / 2048) + EPSILON)
        for f in range(4):
            normed[pl.ds(pl.multiple_of(i * 32, 32), 32), f * 512 : f * 512 + 512] = (
                parts[f] * scale * mix_gain[:, f * 512 : f * 512 + 512]
            ).astype(BF)
        return 0

    lax.fori_loop(0, 16, norm_rows, 0)

    all_colors(turn, 0, 2)
    all_colors(start1, 1, 2)
    all_colors(start1, 2, 1)
    all_colors(finish, 0, 2)

    lane = lax.broadcasted_iota(jnp.int32, (256, 128), 1)
    low_lane = lane < 64
    key_row = jnp.concatenate([key_gain[...], jnp.ones_like(key_gain[...])], axis=1)
    query_row = jnp.concatenate([query_gain[...], query_gain[...]], axis=1)

    def project(s, xi, cols):
        lhs = normed[pl.ds(pl.multiple_of(s * 256, 256), 256), :]
        rhs = w[xi, :, :, :, cols[0] : cols[1]].reshape(2048, cols[1] - cols[0])
        return jnp.dot(lhs, rhs, preferred_element_type=F32)

    def first_part(i, _):
        xi, s = i // 2, lax.rem(i, 2)
        kv = project(s, xi, KV)
        square = jnp.sum(jnp.where(low_lane, kv * kv, 0.0), axis=-1, keepdims=True)
        keyed = kv * lax.rsqrt(square * (1.0 / 64) + EPSILON) * key_row
        kve[s, xi, 128:384, :] = jnp.where(low_lane, keyed, kv).astype(BF)
        value, gate = project(s, xi, CV), project(s, xi, CG)
        gated = (value * jax.nn.sigmoid(gate)).astype(BF).astype(F32)
        ge[s, xi * 2, 16:272, :] = gated[:, :128]
        ge[s, xi * 2 + 1, 16:272, :] = gated[:, 128:]
        return 0

    lax.fori_loop(0, 4, first_part, 0)

    for s in (0, 1):
        for side in (0, 1):
            if side == 0:
                wraps = x == 3
                step = jnp.where(jnp.logical_and(wraps, s == 1), 1, 0)
                to = (lax.rem(q + step, 16) * 2 + k, up(x))
                src_kv, dst_kv, src_ge, dst_ge = (256, 0, 256, 0)
            else:
                wraps = x == 0
                step = jnp.where(jnp.logical_and(wraps, s == 0), 15, 0)
                to = (lax.rem(q + step, 16) * 2 + k, up(x, 3))
                src_kv, dst_kv, src_ge, dst_ge = (128, 384, 16, 272)
            seg = jnp.where(wraps, 1 - s, s)
            i = s * 4 + side * 2
            j = seg * 4 + side * 2
            send(kve.at[s, :, pl.ds(src_kv, 128), :], kve.at[seg, :, pl.ds(dst_kv, 128), :],
                 halo_send.at[i], halo_recv.at[j], to)
            send(ge.at[s, :, pl.ds(src_ge, 16), :], ge.at[seg, :, pl.ds(dst_ge, 16), :],
                 halo_send.at[i + 1], halo_recv.at[j + 1], to)

    all_colors(turn, 2, 1)
    all_colors(turn, 1, 2)
    all_colors(finish, 2, 1)
    all_colors(start1, 2, 2)

    for s in (0, 1):
        for side in (0, 1):
            i = s * 4 + side * 2
            recv(kve.at[s, :, pl.ds(0 if side == 0 else 384, 128), :], halo_send.at[i], halo_recv.at[i])
            recv(ge.at[s, :, pl.ds(0 if side == 0 else 272, 16), :], halo_send.at[i + 1], halo_recv.at[i + 1])
    is_first = jnp.logical_and(q == 0, x == 0)
    is_last = jnp.logical_and(q == 15, x == 3)

    @pl.when(is_first)
    def _():
        ge[0, :, 0:16, :] = jnp.zeros((4, 16, 128), F32)

    @pl.when(is_last)
    def _():
        ge[1, :, 272:288, :] = jnp.zeros((4, 16, 128), F32)

    recv(small.at[1 - xi0], sm_send.at[1], sm_recv.at[1 - xi0])
    recv(small.at[xi0], sm_send.at[1], sm_recv.at[xi0], not_source)

    def conv_block(i, _):
        s, cb = i // 4, lax.rem(i, 4)
        xi, half = cb // 2, lax.rem(cb, 2)
        tap_rows = jnp.where(half == 0, small[xi, :, 0:128], small[xi, :, 128:256])
        for r in (0, 128):
            total = jnp.zeros((128, 128), F32)
            for t in range(31):
                total = total + tap_rows[t : t + 1, :] * ge[s, cb, r + 1 + t : r + 129 + t, :]
            conv[cb, pl.ds(pl.multiple_of(s * 256, 256) + r, 128), :] = total
        return 0

    lax.fori_loop(0, 8, conv_block, 0)

    def stats(i, _):
        rows = pl.ds(pl.multiple_of(i * 64, 64), 64)
        blocks = [conv[cb, rows, :] for cb in range(4)]
        mean = jnp.sum(blocks[0] + blocks[1] + blocks[2] + blocks[3], axis=-1, keepdims=True) * (1.0 / 512)
        dev_sq = sum((b - mean) * (b - mean) for b in blocks)
        m2 = jnp.sum(dev_sq, axis=-1, keepdims=True)
        stat_own[rows, :] = jnp.where(low_lane[:64], mean, m2)
        return 0

    lax.fori_loop(0, 8, stats, 0)
    send(stat_own, stat_peer, stat_send.at[0], stat_recv.at[0], peer)

    all_colors(finish, 1, 2)

    def query_part(i, _):
        xi, s = i // 2, lax.rem(i, 2)
        full = project(s, xi, Q)
        for pair in (0, 1):
            v = full[:, pair * 128 : pair * 128 + 128]
            sq = v * v
            even = jnp.sum(jnp.where(low_lane, sq, 0.0), axis=-1, keepdims=True)
            odd = jnp.sum(jnp.where(low_lane, 0.0, sq), axis=-1, keepdims=True)
            scale = lax.rsqrt(jnp.where(low_lane, even, odd) * (1.0 / 64) + EPSILON)
            rounded = (v * scale * query_row).astype(BF).astype(F32) * 0.125
            qn[xi * 2 + pair, pl.ds(pl.multiple_of(s * 256, 256), 256), :] = rounded.astype(BF)
        return 0

    lax.fori_loop(0, 4, query_part, 0)
    all_colors(turn, 2, 2)

    row_i = lax.rem(lax.broadcasted_iota(jnp.int32, (256, 384), 0), 128)
    col_i = lax.broadcasted_iota(jnp.int32, (256, 384), 1)
    lane384 = lax.broadcasted_iota(jnp.int32, (384, 128), 1) < 64

    def attention(i, _):
        xi, s, b = i // 4, lax.rem(i // 2, 2), lax.rem(i, 2)
        base = pl.multiple_of(s * 256 + b * 128, 128)
        kv = kve[s, xi, pl.ds(pl.multiple_of(b * 128, 128), 384), :].astype(F32)
        swapped = pltpu.roll(kv, 64, 1)
        first = jnp.where(jnp.logical_and(is_first, s == 0), 128, 0) - b * 128
        end = jnp.where(jnp.logical_and(is_last, s == 1), 384, 512) - b * 128
        reach = col_i - row_i
        allowed = (reach >= 0) & (reach <= 256) & (col_i >= first) & (col_i < end)
        q01 = qn[xi * 2, pl.ds(base, 128), :].astype(F32)
        q23 = qn[xi * 2 + 1, pl.ds(base, 128), :].astype(F32)
        both = jnp.concatenate([q01, q23], axis=0)
        even = jnp.where(low_lane, both, 0.0).astype(BF)
        odd = jnp.where(low_lane, 0.0, both).astype(BF)
        nt = (((1,), (1,)), ((), ()))

        def mix(heads, keys, values):
            scores = lax.dot_general(heads, keys.astype(BF), nt, preferred_element_type=F32)
            weights = jnp.where(allowed, jnp.exp(scores), 0.0).astype(BF)
            return jnp.dot(weights, values.astype(BF), preferred_element_type=F32)

        o_even = mix(even, kv, jnp.where(lane384, swapped, 1.0))
        o_odd = mix(odd, swapped, jnp.where(lane384, 1.0, kv))
        number = jnp.where(low_lane, o_even, o_odd)
        weight = pltpu.roll(jnp.where(low_lane, o_odd, o_even), 64, 1)
        sink = jnp.exp(small[xi, 32:33, :])
        feats[xi, pl.ds(base, 128), 0:128] = (number[:128] / (weight[:128] + sink[:, :128])).astype(BF)
        feats[xi, pl.ds(base, 128), 128:256] = (number[128:] / (weight[128:] + sink[:, 128:])).astype(BF)
        return 0

    lax.fori_loop(0, 8, attention, 0)

    recv(stat_peer, stat_send.at[0], stat_recv.at[0])

    def feature(i, _):
        rows = pl.ds(pl.multiple_of(i * 64, 64), 64)
        a, b = stat_own[rows, :], stat_peer[rows, :]
        mean = 0.5 * (a[:, 0:1] + b[:, 0:1])
        gap = a[:, 0:1] - b[:, 0:1]
        spread = (a[:, 64:65] + b[:, 64:65] + gap * gap * 256.0) * (1.0 / 1024)
        scale = lax.rsqrt(spread + EPSILON)
        for cb in range(4):
            xi, half = cb // 2, cb % 2
            gain = small[xi, 31:32, half * 128 : half * 128 + 128]
            v = (conv[cb, rows, :] - mean) * scale * gain
            feats[xi, rows, 256 + half * 128 : 384 + half * 128] = (v * jax.nn.sigmoid(v)).astype(BF)
        return 0

    lax.fori_loop(0, 8, feature, 0)
    all_colors(finish, 2, 2)

    mine_rows = pl.ds(pl.multiple_of(k * 256, 256), 256)
    other_rows = pl.ds(pl.multiple_of((1 - k) * 256, 256), 256)
    for nb in range(8):
        zz, y0 = nb // 2, (nb % 2) * 2
        rhs = [jnp.concatenate([p[xi, zz, y0], p[xi, zz, y0 + 1]], axis=1) for xi in (0, 1)]
        part_send[nb] = sum(
            jnp.dot(feats[xi, other_rows, :], rhs[xi], preferred_element_type=F32) for xi in (0, 1)
        ).astype(BF)
        send(part_send.at[nb], part_recv.at[nb], out_send.at[nb], out_recv.at[nb], peer)
        part_own[nb] = sum(
            jnp.dot(feats[xi, mine_rows, :], rhs[xi], preferred_element_type=F32) for xi in (0, 1)
        )
    for nb in range(8):
        recv(part_recv.at[nb], out_send.at[nb], out_recv.at[nb])
        out[:, nb * 256 : nb * 256 + 256] = (part_own[nb] + part_recv[nb].astype(F32)).astype(BF)

    for src, dst, ssem, rsem, device, cond in sends:
        def done(src=src, dst=dst, ssem=ssem, rsem=rsem, device=device):
            copy(src, dst, ssem, rsem, device).wait_send()

        if cond is None:
            done()
        else:
            pl.when(cond)(done)


def on_device(tokens, mix_gain, wq, wk, wv, wcv, wcg, query_gain, key_gain, sinks, taps, conv_gain, attn_proj, conv_proj):
    vmem = pl.BlockSpec(memory_space=pltpu.VMEM)
    dma = pltpu.SemaphoreType.DMA
    return pl.pallas_call(
        kernel,
        out_shape=jax.ShapeDtypeStruct((256, 2048), BF),
        in_specs=[pl.BlockSpec(memory_space=pl.ANY)] + [vmem] * 13,
        out_specs=vmem,
        scratch_shapes=[
            pltpu.VMEM((2, 4, 4, 128, 896), BF),
            pltpu.VMEM((2, 4, 4, 512, 128), BF),
            pltpu.VMEM((64, 896), BF),
            pltpu.VMEM((256, 128), BF),
            pltpu.VMEM((256, 128), BF),
            pltpu.VMEM((2, 40, 256), F32),
            pltpu.VMEM((2, 4, 256, 512), BF),
            pltpu.VMEM((512, 2048), BF),
            pltpu.VMEM((4, 512, 128), BF),
            pltpu.VMEM((2, 2, 512, 128), BF),
            pltpu.VMEM((2, 4, 288, 128), F32),
            pltpu.VMEM((4, 512, 128), F32),
            pltpu.VMEM((512, 128), F32),
            pltpu.VMEM((512, 128), F32),
            pltpu.VMEM((2, 512, 512), BF),
            pltpu.VMEM((8, 256, 256), F32),
            pltpu.VMEM((8, 256, 256), BF),
            pltpu.VMEM((8, 256, 256), BF),
            dma((108,)), dma((108,)), dma((2,)), dma((2,)), dma((4,)), dma((4,)), dma((4,)), dma((4,)), dma(()),
            dma((4,)), dma((2,)), dma((8,)), dma((8,)), dma((1,)), dma((1,)), dma((8,)), dma((8,)),
        ],
        compiler_params=pltpu.CompilerParams(
            collective_id=0, has_side_effects=True, vmem_limit_bytes=60 * 1024 * 1024
        ),
        name="layer",
    )(
        tokens, mix_gain.reshape(1, -1), wq, wk, wv, wcv, wcg, query_gain.reshape(1, -1), key_gain.reshape(1, -1),
        jnp.repeat(sinks, 64).reshape(1, -1), taps, conv_gain.reshape(1, -1), attn_proj, conv_proj,
    )


def solution(mesh):
    placed = (
        P("sp", "tp"), P(), P("sp", "tp"), P("sp", "tp"), P("sp", "tp"), P("sp", "tp"), P("sp", "tp"),
        P(), P(), P("tp"), P(None, "tp"), P("tp"), P("tp", "sp"), P("tp", "sp"),
    )
    return jax.shard_map(
        on_device, mesh=mesh, in_specs=placed, out_specs=P(("sp", "tp"), None), check_vma=False
    )
```

```python
import jax
import jax.numpy as jnp
from jax import lax
from jax.experimental import pallas as pl
from jax.experimental.pallas import tpu as pltpu
from jax.sharding import PartitionSpec as P

MESH = pl.DeviceIdType.MESH
EPSILON = 0.1
BF = jnp.bfloat16
F32 = jnp.float32

CV, CG, Q, KV = (0, 256), (256, 512), (512, 768), (768, 896)
STAGES = (
    ("w", 0, 512, ((0, 48, 32), (48, 32, 16), (80, 48, 32))),
    ("w", 512, 384, ((0, 48, 32), (48, 32, 16), (80, 48, 32))),
    ("p", 0, 128, ((0, 144, 80), (144, 176, 96), (320, 192, 96))),
)
ORDERS = ("xyz", "yzx", "xzy")


def kernel(
    tokens, *rest,
):
    given, (out, *held), rest = rest[:13], rest[13:27], rest[27:]
    mix_gain, wq, wk, wv, wcv, wcg, query_gain, key_gain, sinks, taps, conv_gain, attn_proj, conv_proj = held
    (
        w, p, mine_w, mine_p, peer_p, small, hop, edge_send, edge_recv, x_buf, normed, qn, kve, ge, conv, stat_own,
        stat_peer, feats, part_own, part_send, part_recv,
        load_sem, ag_send, ag_recv, d2d_send, d2d_recv, tok_send, tok_recv, hop_send, hop_recv, fwd_send, fwd_recv,
        loc_sem, sm_send, sm_recv, halo_send, halo_recv, stat_send, stat_recv, out_send, out_recv,
    ) = rest
    loads = [pltpu.make_async_copy(a, b, load_sem.at[i]) for i, (a, b) in enumerate(zip(given, held))]
    for load in loads:
        load.start()
    sp, x = lax.axis_index("sp"), lax.axis_index("tp")
    k = lax.rem(sp, 2)
    q = sp // 2
    y, z = lax.rem(q, 4), q // 4
    pos = lax.rem(x + 4 - 2 * k, 4)
    xi0 = lax.rem(x, 2)
    is_source = pos < 2
    bufs = {"w": w, "p": p}

    def dev(xx, yy, zz, kk):
        return (zz * 8 + yy * 2 + kk, xx)

    def up(v, n=1):
        return lax.rem(v + n, 4)

    peer = dev(x, y, z, 1 - k)
    sends = []

    def copy(src, dst, ssem, rsem, device):
        return pltpu.make_async_remote_copy(
            src_ref=src, dst_ref=dst, send_sem=ssem, recv_sem=rsem, device_id=device, device_id_type=MESH
        )

    def send(src, dst, ssem, rsem, device, cond=None):
        def go():
            copy(src, dst, ssem, rsem, device).start()

        if cond is None:
            go()
        else:
            pl.when(cond)(go)
        sends.append((src, dst, ssem, rsem, device, cond))

    def recv(dst, ssem, rsem, cond=None):
        def go():
            copy(dst, dst, ssem, rsem, peer).wait_recv()

        if cond is None:
            go()
        else:
            pl.when(cond)(go)

    def ref_of(stage, color, phase, where, half):
        name, c0, cn, rows = STAGES[stage]
        buf = bufs[name]
        r0, rn, rh = rows[color]
        cols = pl.ds(c0, cn)
        rr = pl.ds(r0, rn)
        parts = {None: rr, 0: pl.ds(r0, rh), 1: pl.ds(r0 + rh, rn - rh)}
        two = {None: slice(None), 0: pl.ds(0, 2), 1: pl.ds(2, 2)}
        one = {None: slice(None), 0: pl.ds(0, 1), 1: pl.ds(1, 1)}
        axis = ORDERS[color][phase]
        if phase == 0:
            if axis == "x":
                return buf.at[where, z, y, parts[half], cols]
            if axis == "y":
                return buf.at[xi0, z, where, parts[half], cols]
            return buf.at[xi0, where, y, parts[half], cols]
        if color == 0:
            if axis == "y":
                return buf.at[one[half], z, where, rr, cols]
            return buf.at[one[half], where, :, rr, cols]
        if color == 1:
            if axis == "z":
                return buf.at[xi0, where, two[half], rr, cols]
            return buf.at[where, two[half], :, rr, cols]
        if axis == "z":
            return buf.at[one[half], where, y, rr, cols]
        return buf.at[one[half], :, where, rr, cols]

    def context(stage, color, phase):
        axis = ORDERS[color][phase]
        base = ((stage * 3 + color) * 3 + phase) * 4
        ss = [ag_send.at[base + i] for i in range(4)]
        rs = [ag_recv.at[base + i] for i in range(4)]
        only_sources = is_source if ORDERS[color].index("x") > phase else None
        return axis, ss, rs, only_sources

    def ring(axis):
        if axis == "y":
            return y, dev(x, up(y), z, k), dev(x, up(y, 3), z, k)
        return z, dev(x, y, up(z), k), dev(x, y, up(z, 3), k)

    def start1(stage, color, phase):
        axis, ss, rs, cond = context(stage, color, phase)
        if axis == "x":
            r = ref_of(stage, color, phase, xi0, None)
            send(r, r, ss[0], rs[0], dev(up(x), y, z, k), is_source)
            send(r, r, ss[1], rs[0], dev(up(x, 3), y, z, k), is_source)
        else:
            at, right, left = ring(axis)
            r = ref_of(stage, color, phase, at, None)
            send(r, r, ss[0], rs[0], right, cond)
            send(r, r, ss[1], rs[1], left, cond)

    def turn(stage, color, phase):
        axis, ss, rs, cond = context(stage, color, phase)
        if axis == "x":
            other = 1 - xi0
            recv(ref_of(stage, color, phase, other, None), ss[0], rs[0])
            h0 = ref_of(stage, color, phase, other, 0)
            h1 = ref_of(stage, color, phase, other, 1)
            to_low = dev(jnp.where(pos == 0, up(x, 3), up(x)), y, z, k)
            to_high = dev(jnp.where(pos == 2, up(x), up(x, 3)), y, z, k)
            send(h0, h0, ss[2], rs[2], to_low, pos < 2)
            send(h1, h1, ss[3], rs[3], to_high, pos >= 2)
        else:
            at, right, left = ring(axis)
            recv(ref_of(stage, color, phase, up(at, 3), None), ss[0], rs[0], cond)
            h0 = ref_of(stage, color, phase, up(at, 3), 0)
            send(h0, h0, ss[2], rs[2], right, cond)
            recv(ref_of(stage, color, phase, up(at), None), ss[1], rs[1], cond)
            h1 = ref_of(stage, color, phase, up(at), 1)
            send(h1, h1, ss[3], rs[3], left, cond)

    def finish(stage, color, phase):
        axis, ss, rs, cond = context(stage, color, phase)
        if axis == "x":
            recv(ref_of(stage, color, phase, xi0, 0), ss[2], rs[2], pos >= 2)
            recv(ref_of(stage, color, phase, xi0, 1), ss[3], rs[3], pos >= 2)
        else:
            at, _, _ = ring(axis)
            recv(ref_of(stage, color, phase, up(at, 2), 0), ss[2], rs[2], cond)
            recv(ref_of(stage, color, phase, up(at, 2), 1), ss[3], rs[3], cond)

    def all_colors(step, stage, phase):
        for color in range(3):
            step(stage, color, phase)

    def flush(count=None):
        for _ in range(len(sends) if count is None else count):
            src, dst, ssem, rsem, device, cond = sends.pop(0)

            def done():
                copy(src, dst, ssem, rsem, device).wait_send()

            if cond is None:
                done()
            else:
                pl.when(cond)(done)

    own_rows = pl.ds(pl.multiple_of(k * 64, 64), 64)
    barrier = pltpu.get_barrier_semaphore()
    y_up, z_up = up(y), up(z)
    partners = [
        peer, dev(up(x), y, z, k), dev(up(x, 3), y, z, k),
        dev(x, y_up, z, k), dev(x, up(y, 3), z, k), dev(x, y, z_up, k), dev(x, y, up(z, 3), k),
    ]
    for partner in partners:
        pl.semaphore_signal(barrier, inc=1, device_id=partner, device_id_type=MESH)
    own = pl.multiple_of(x * 256, 256)
    local = pltpu.make_async_copy(tokens.at[pl.ds(own, 256), :], x_buf.at[k, x], loc_sem)
    local.start()
    for load in loads:
        load.wait()
    shard = jnp.concatenate([wcv[...], wcg[...], wq[...], wk[...], wv[...]], axis=1)

    @pl.when(is_source)
    def _():
        w[xi0, z, y, own_rows, :] = shard

    @pl.when(jnp.logical_not(is_source))
    def _():
        mine_w[...] = shard

    mine_p[...] = jnp.concatenate([attn_proj[...], conv_proj[...]], axis=0)
    small[xi0, 0:31, :] = taps[...]
    small[xi0, 31:32, :] = conv_gain[...]
    small[xi0, 32:33, :] = jnp.concatenate(
        [jnp.broadcast_to(sinks[:, h : h + 1], (1, 64)) for h in range(4)], axis=1
    )

    pl.semaphore_wait(barrier, len(partners))

    not_source = jnp.logical_not(is_source)
    slot = w.at[xi0, z, y, own_rows, :]
    send(mine_w, slot, d2d_send.at[0], d2d_recv.at[0], peer, not_source)
    send(mine_p, peer_p, d2d_send.at[1], d2d_recv.at[1], peer)
    peer_rows = pl.ds(pl.multiple_of((1 - k) * 64, 64), 64)
    recv(w.at[xi0, z, y, peer_rows, :], d2d_send.at[0], d2d_recv.at[0], is_source)
    all_colors(start1, 0, 0)
    all_colors(start1, 1, 0)

    right, left, across = dev(up(x), y, z, k), dev(up(x, 3), y, z, k), up(x, 2)

    def token_sends():
        for to, device, i in ((up(x), right, 0), (up(x, 3), left, 1)):
            far = tokens.at[pl.ds(pl.multiple_of(across * 256 + i * 128, 128), 128), :]
            send(far, hop.at[i], hop_send.at[i], hop_recv.at[i], device)
            near = tokens.at[pl.ds(pl.multiple_of(to * 256, 256), 256), :]
            send(near, x_buf.at[k, x], tok_send.at[i], tok_recv.at[i], device)

    def token_hops():
        for origin, device, i in ((up(x, 3), right, 0), (up(x), left, 1)):
            recv(hop.at[i], hop_send.at[i], hop_recv.at[i])
            send(hop.at[i], x_buf.at[k, origin, pl.ds(i * 128, 128), :], tok_send.at[2 + i], tok_recv.at[2 + i], device)

    def tokens_on():
        for i, origin in ((0, up(x, 3)), (1, up(x))):
            recv(x_buf.at[k, origin], tok_send.at[i], tok_recv.at[i])
            send(x_buf.at[k, origin], x_buf.at[k, origin], fwd_send.at[1 + i], fwd_recv.at[1 + i], peer)
        for i in (0, 1):
            recv(x_buf.at[k, across, pl.ds(i * 128, 128), :], tok_send.at[2 + i], tok_recv.at[2 + i])
        send(x_buf.at[k, across], x_buf.at[k, across], fwd_send.at[3], fwd_recv.at[3], peer)

    def small_on():
        recv(small.at[1 - xi0], sm_send.at[0], sm_recv.at[1 - xi0])
        beyond = dev(jnp.where(jnp.logical_or(pos == 0, pos == 3), up(x, 3), up(x)), y, z, k)
        send(small.at[1 - xi0], small.at[1 - xi0], sm_send.at[2], sm_recv.at[1 - xi0], beyond, is_source)

    recv(peer_p, d2d_send.at[1], d2d_recv.at[1])

    @pl.when(is_source)
    def _():
        a, b = mine_p[...], peer_p[...]
        low = jnp.where(k == 0, a, b)
        high = jnp.where(k == 0, b, a)
        p[xi0, z, y, 0:256, :] = jnp.concatenate([low[:64], high[:64]], axis=0).T
        p[xi0, z, y, 256:512, :] = jnp.concatenate([low[64:], high[64:]], axis=0).T

    all_colors(turn, 0, 0)
    all_colors(turn, 1, 0)
    all_colors(start1, 2, 0)
    token_sends()
    send(tokens.at[pl.ds(own, 256), :], x_buf.at[k, x], fwd_send.at[0], fwd_recv.at[0], peer)
    mine_small = small.at[xi0]
    for i, device in enumerate((right, left)):
        send(mine_small, mine_small, sm_send.at[i], sm_recv.at[xi0], device, is_source)
    all_colors(finish, 0, 0)
    all_colors(start1, 0, 1)
    all_colors(finish, 1, 0)
    all_colors(start1, 1, 1)
    all_colors(turn, 2, 0)
    all_colors(turn, 0, 1)
    all_colors(turn, 1, 1)
    all_colors(finish, 2, 0)
    all_colors(start1, 2, 1)
    token_hops()
    all_colors(finish, 0, 1)
    early = len(sends)
    all_colors(start1, 0, 2)
    small_on()
    all_colors(finish, 1, 1)
    tokens_on()
    local.wait()
    recv(x_buf.at[1 - k, x], fwd_send.at[0], fwd_recv.at[0])
    for i, origin in ((1, up(x, 3)), (2, up(x)), (3, across)):
        recv(x_buf.at[1 - k, origin], fwd_send.at[i], fwd_recv.at[i])

    def norm_rows(i, _):
        s, r = i // 8, lax.rem(i, 8)
        rows = pl.ds(pl.multiple_of(r * 32, 32), 32)
        parts = [x_buf[s, f, rows, :].astype(F32) for f in range(4)]
        square = sum(jnp.sum(v * v, axis=-1, keepdims=True) for v in parts)
        scale = lax.rsqrt(square * (1.0 / 2048) + EPSILON)
        for f in range(4):
            normed[pl.ds(pl.multiple_of(i * 32, 32), 32), f * 512 : f * 512 + 512] = (
                parts[f] * scale * mix_gain[:, f * 512 : f * 512 + 512]
            ).astype(BF)
        return 0

    lax.fori_loop(0, 16, norm_rows, 0)

    all_colors(turn, 0, 2)
    all_colors(turn, 2, 1)
    all_colors(start1, 1, 2)
    flush(early)
    all_colors(finish, 0, 2)

    lane = lax.broadcasted_iota(jnp.int32, (256, 128), 1)
    low_lane = lane < 64
    key_row = jnp.concatenate([key_gain[...], jnp.ones_like(key_gain[...])], axis=1)
    query_row = jnp.concatenate([query_gain[...], query_gain[...]], axis=1)

    def project(s, xi, cols):
        lhs = normed[pl.ds(pl.multiple_of(s * 256, 256), 256), :]
        rhs = w[xi, :, :, :, cols[0] : cols[1]].reshape(2048, cols[1] - cols[0])
        return jnp.dot(lhs, rhs, preferred_element_type=F32)

    def gated_part(i, _):
        xi, s = i // 2, lax.rem(i, 2)
        value, gate = project(s, xi, CV), project(s, xi, CG)
        rounded = (value * jax.nn.sigmoid(gate)).astype(BF)
        gated = rounded.astype(F32)
        for half in (0, 1):
            lanes = slice(half * 128, half * 128 + 128)
            ge[s, xi * 2 + half, 16:272, :] = gated[:, lanes]
            edge_send[s, 0, xi * 2 + half] = rounded[240:, lanes]
            edge_send[s, 1, xi * 2 + half] = rounded[:16, lanes]
        return 0

    lax.fori_loop(0, 4, gated_part, 0)

    def neighbour(s, side):
        wraps, over = (x == 3, 1) if side == 0 else (x == 0, 15)
        step = jnp.where(jnp.logical_and(wraps, s == 1 - side), over, 0)
        return (lax.rem(q + step, 16) * 2 + k, up(x, 1 if side == 0 else 3)), jnp.where(wraps, 1 - s, s)

    SIDES = ((0, 0), (0, 1), (1, 0), (1, 1))
    is_first = jnp.logical_and(q == 0, x == 0)
    is_last = jnp.logical_and(q == 15, x == 3)

    for s, side in SIDES:
        to, seg = neighbour(s, side)
        send(edge_send.at[s, side], edge_recv.at[seg, side], halo_send.at[4 + s * 2 + side],
             halo_recv.at[4 + seg * 2 + side], to)
    all_colors(finish, 2, 1)
    all_colors(turn, 1, 2)
    all_colors(start1, 2, 2)
    recv(small.at[xi0], sm_send.at[0], sm_recv.at[xi0], not_source)
    for s, side in SIDES:
        recv(edge_recv.at[s, side], halo_send.at[4], halo_recv.at[4 + s * 2 + side])
        ge[s, :, side * 272 : side * 272 + 16, :] = edge_recv[s, side].astype(F32)

    @pl.when(is_first)
    def _():
        ge[0, :, 0:16, :] = jnp.zeros((4, 16, 128), F32)

    @pl.when(is_last)
    def _():
        ge[1, :, 272:288, :] = jnp.zeros((4, 16, 128), F32)

    def conv_block(i, _):
        s, cb = i // 4, lax.rem(i, 4)
        xi, half = cb // 2, lax.rem(cb, 2)
        tap_rows = jnp.where(half == 0, small[xi, :, 0:128], small[xi, :, 128:256])
        for r in (0, 128):
            total = jnp.zeros((128, 128), F32)
            for t in range(31):
                total = total + tap_rows[t : t + 1, :] * ge[s, cb, r + 1 + t : r + 129 + t, :]
            conv[cb, pl.ds(pl.multiple_of(s * 256, 256) + r, 128), :] = total
        return 0

    lax.fori_loop(0, 8, conv_block, 0)

    def stats(i, _):
        rows = pl.ds(pl.multiple_of(i * 64, 64), 64)
        blocks = [conv[cb, rows, :] for cb in range(4)]
        mean = jnp.sum(blocks[0] + blocks[1] + blocks[2] + blocks[3], axis=-1, keepdims=True) * (1.0 / 512)
        dev_sq = sum((b - mean) * (b - mean) for b in blocks)
        m2 = jnp.sum(dev_sq, axis=-1, keepdims=True)
        stat_own[rows, :] = jnp.where(low_lane[:64], mean, m2)
        return 0

    lax.fori_loop(0, 8, stats, 0)
    send(stat_own, stat_peer, stat_send.at[0], stat_recv.at[0], peer)

    all_colors(finish, 1, 2)

    def first_part(i, _):
        xi, s = i // 2, lax.rem(i, 2)
        kv = project(s, xi, KV)
        square = jnp.sum(jnp.where(low_lane, kv * kv, 0.0), axis=-1, keepdims=True)
        keyed = kv * lax.rsqrt(square * (1.0 / 64) + EPSILON) * key_row
        kve[s, xi, 128:384, :] = jnp.where(low_lane, keyed, kv).astype(BF)
        return 0

    lax.fori_loop(0, 4, first_part, 0)
    for s, side in SIDES:
        to, seg = neighbour(s, side)
        src, dst = (256, 0) if side == 0 else (128, 384)
        send(kve.at[s, :, pl.ds(src, 128), :], kve.at[seg, :, pl.ds(dst, 128), :],
             halo_send.at[s * 2 + side], halo_recv.at[seg * 2 + side], to)
    def query_part(i, _):
        xi, s = i // 2, lax.rem(i, 2)
        full = project(s, xi, Q)
        for pair in (0, 1):
            v = full[:, pair * 128 : pair * 128 + 128]
            sq = v * v
            even = jnp.sum(jnp.where(low_lane, sq, 0.0), axis=-1, keepdims=True)
            odd = jnp.sum(jnp.where(low_lane, 0.0, sq), axis=-1, keepdims=True)
            scale = lax.rsqrt(jnp.where(low_lane, even, odd) * (1.0 / 64) + EPSILON)
            rounded = (v * scale * query_row).astype(BF).astype(F32) * 0.125
            qn[xi * 2 + pair, pl.ds(pl.multiple_of(s * 256, 256), 256), :] = rounded.astype(BF)
        return 0

    lax.fori_loop(0, 4, query_part, 0)
    recv(stat_peer, stat_send.at[0], stat_recv.at[0])

    def feature(i, _):
        rows = pl.ds(pl.multiple_of(i * 64, 64), 64)
        a, b = stat_own[rows, :], stat_peer[rows, :]
        mean = 0.5 * (a[:, 0:1] + b[:, 0:1])
        gap = a[:, 0:1] - b[:, 0:1]
        spread = (a[:, 64:65] + b[:, 64:65] + gap * gap * 256.0) * (1.0 / 1024)
        scale = lax.rsqrt(spread + EPSILON)
        for cb in range(4):
            xi, half = cb // 2, cb % 2
            gain = small[xi, 31:32, half * 128 : half * 128 + 128]
            v = (conv[cb, rows, :] - mean) * scale * gain
            feats[rows, xi * 512 + 256 + half * 128 : xi * 512 + 384 + half * 128] = (v * jax.nn.sigmoid(v)).astype(BF)
        return 0

    lax.fori_loop(0, 8, feature, 0)
    all_colors(turn, 2, 2)
    for s, side in SIDES:
        recv(kve.at[s, :, pl.ds(0 if side == 0 else 384, 128), :], halo_send.at[0], halo_recv.at[s * 2 + side])

    row_i = lax.rem(lax.broadcasted_iota(jnp.int32, (256, 384), 0), 128)
    col_i = lax.broadcasted_iota(jnp.int32, (256, 384), 1)
    lane384 = lax.broadcasted_iota(jnp.int32, (384, 128), 1) < 64

    def attention(i, _):
        xi, s, b = i // 4, lax.rem(i // 2, 2), lax.rem(i, 2)
        base = pl.multiple_of(s * 256 + b * 128, 128)
        kv = kve[s, xi, pl.ds(pl.multiple_of(b * 128, 128), 384), :].astype(F32)
        swapped = pltpu.roll(kv, 64, 1)
        first = jnp.where(jnp.logical_and(is_first, s == 0), 128, 0) - b * 128
        end = jnp.where(jnp.logical_and(is_last, s == 1), 384, 512) - b * 128
        reach = col_i - row_i
        allowed = (reach >= 0) & (reach <= 256) & (col_i >= first) & (col_i < end)
        q01 = qn[xi * 2, pl.ds(base, 128), :].astype(F32)
        q23 = qn[xi * 2 + 1, pl.ds(base, 128), :].astype(F32)
        both = jnp.concatenate([q01, q23], axis=0)
        even = jnp.where(low_lane, both, 0.0).astype(BF)
        odd = jnp.where(low_lane, 0.0, both).astype(BF)
        nt = (((1,), (1,)), ((), ()))

        def mix(heads, keys, values):
            scores = lax.dot_general(heads, keys.astype(BF), nt, preferred_element_type=F32)
            weights = jnp.where(allowed, jnp.exp(scores), 0.0).astype(BF)
            return jnp.dot(weights, values.astype(BF), preferred_element_type=F32)

        o_even = mix(even, kv, jnp.where(lane384, swapped, 1.0))
        o_odd = mix(odd, swapped, jnp.where(lane384, 1.0, kv))
        number = jnp.where(low_lane, o_even, o_odd)
        weight = pltpu.roll(jnp.where(low_lane, o_odd, o_even), 64, 1)
        sink = jnp.exp(small[xi, 32:33, :])
        col = pl.multiple_of(xi * 512, 512)
        feats[pl.ds(base, 128), pl.ds(col, 128)] = (number[:128] / (weight[:128] + sink[:, :128])).astype(BF)
        feats[pl.ds(base, 128), pl.ds(col + 128, 128)] = (number[128:] / (weight[128:] + sink[:, 128:])).astype(BF)
        return 0

    lax.fori_loop(0, 8, attention, 0)

    all_colors(finish, 2, 2)

    for nb in range(8):
        zz, y0 = nb // 2, (nb % 2) * 2
        rhs = jnp.concatenate(
            [jnp.concatenate([p[xi, zz, y0], p[xi, zz, y0 + 1]], axis=1) for xi in (0, 1)], axis=0
        )
        part = jnp.dot(feats[...], rhs, preferred_element_type=F32).reshape(2, 256, 256)
        part_send[nb] = part.astype(BF)
        send(part_send.at[nb, 1 - k], part_recv.at[nb], out_send.at[nb], out_recv.at[nb], peer)
        part_own[nb] = part
    for nb in range(8):
        recv(part_recv.at[nb], out_send.at[nb], out_recv.at[nb])
        out[:, nb * 256 : nb * 256 + 256] = (part_own[nb, k] + part_recv[nb].astype(F32)).astype(BF)
    flush()


def on_device(tokens, mix_gain, wq, wk, wv, wcv, wcg, query_gain, key_gain, sinks, taps, conv_gain, attn_proj, conv_proj):
    vmem = pl.BlockSpec(memory_space=pltpu.VMEM)
    dma = pltpu.SemaphoreType.DMA
    arrays = (
        tokens, mix_gain.reshape(1, -1), wq, wk, wv, wcv, wcg, query_gain.reshape(1, -1), key_gain.reshape(1, -1),
        sinks.reshape(1, -1), taps, conv_gain.reshape(1, -1), attn_proj.T, conv_proj.T,
    )
    return pl.pallas_call(
        kernel,
        out_shape=jax.ShapeDtypeStruct((256, 2048), BF),
        in_specs=[pl.BlockSpec(memory_space=pltpu.HBM)] * 14,
        out_specs=vmem,
        scratch_shapes=[
            *(pltpu.VMEM(a.shape, a.dtype) for a in arrays[1:]),
            pltpu.VMEM((2, 4, 4, 128, 896), BF),
            pltpu.VMEM((2, 4, 4, 512, 128), BF),
            pltpu.VMEM((64, 896), BF),
            pltpu.VMEM((128, 256), BF),
            pltpu.VMEM((128, 256), BF),
            pltpu.VMEM((2, 40, 256), F32),
            pltpu.VMEM((2, 128, 512), BF),
            pltpu.VMEM((2, 2, 4, 16, 128), BF),
            pltpu.VMEM((2, 2, 4, 16, 128), BF),
            pltpu.VMEM((2, 4, 256, 512), BF),
            pltpu.VMEM((512, 2048), BF),
            pltpu.VMEM((4, 512, 128), BF),
            pltpu.VMEM((2, 2, 512, 128), BF),
            pltpu.VMEM((2, 4, 288, 128), F32),
            pltpu.VMEM((4, 512, 128), F32),
            pltpu.VMEM((512, 128), F32),
            pltpu.VMEM((512, 128), F32),
            pltpu.VMEM((512, 1024), BF),
            pltpu.VMEM((8, 2, 256, 256), F32),
            pltpu.VMEM((8, 2, 256, 256), BF),
            pltpu.VMEM((8, 256, 256), BF),
            dma((13,)), dma((108,)), dma((108,)), dma((2,)), dma((2,)), dma((4,)), dma((4,)), dma((2,)), dma((2,)), dma((4,)), dma((4,)), dma(()),
            dma((4,)), dma((2,)), dma((8,)), dma((8,)), dma((1,)), dma((1,)), dma((8,)), dma((8,)),
        ],
        compiler_params=pltpu.CompilerParams(
            collective_id=0, has_side_effects=True, vmem_limit_bytes=62 * 1024 * 1024
        ),
        name="layer",
    )(*arrays)


def solution(mesh):
    placed = (
        P("sp", "tp"), P(), P("sp", "tp"), P("sp", "tp"), P("sp", "tp"), P("sp", "tp"), P("sp", "tp"),
        P(), P(), P("tp"), P(None, "tp"), P("tp"), P("tp", "sp"), P("tp", "sp"),
    )
    return jax.shard_map(
        on_device, mesh=mesh, in_specs=placed, out_specs=P(("sp", "tp"), None), check_vma=False
    )
```

```python
import jax
import jax.numpy as jnp
from jax import lax
from jax.experimental import pallas as pl
from jax.experimental.pallas import tpu as pltpu
from jax.sharding import PartitionSpec as P

MESH = pl.DeviceIdType.MESH
EPSILON = 0.1
BF = jnp.bfloat16
F32 = jnp.float32

CV, CG, Q, KV = (0, 256), (256, 512), (512, 768), (768, 896)
STAGES = (
    ("w", 0, 512, ((0, 48, 32), (48, 32, 16), (80, 48, 32))),
    ("w", 512, 384, ((0, 48, 32), (48, 32, 16), (80, 48, 32))),
    ("p", 0, 128, ((0, 176, 96), (176, 160, 80), (336, 176, 96))),
)
ORDERS = ("xyz", "yzx", "zxy")
SLOTS = {(False, True): range(2), (False, False): range(3), (True, True): range(4), (True, False): range(6)}
SLOT_COUNT = 3 * sum(
    len(SLOTS[phase > 0, axis == "x"]) for order in ORDERS for phase, axis in enumerate(order)
)
POOL = 112


def kernel(
    tokens, *rest,
):
    given, (out, *held), rest = rest[:13], rest[13:27], rest[27:]
    mix_gain, wq, wk, wv, wcv, wcg, query_gain, key_gain, sinks, taps, conv_gain, attn_proj, conv_proj = held
    (
        w, p, mine_w, mine_p, peer_p, small, hop, edge_send, edge_recv, x_buf, normed, qn, kve, ge, conv, stat_own,
        stat_peer, feats, part_own, part_send, part_recv,
        load_sem, pool, ag_recv, d2d_recv, tok_recv, hop_recv, fwd_recv, loc_sem, sm_recv, halo_recv, stat_recv,
        out_recv,
    ) = rest
    loads = [pltpu.make_async_copy(a, b, load_sem.at[i]) for i, (a, b) in enumerate(zip(given, held))]
    for load in loads:
        load.start()
    sp, x = lax.axis_index("sp"), lax.axis_index("tp")
    k = lax.rem(sp, 2)
    q = sp // 2
    y, z = lax.rem(q, 4), q // 4
    pos = lax.rem(x + 4 - 2 * k, 4)
    xi0 = lax.rem(x, 2)
    is_source = pos < 2
    bufs = {"w": w, "p": p}

    def dev(xx, yy, zz, kk):
        return (zz * 8 + yy * 2 + kk, xx)

    def up(v, n=1):
        return lax.rem(v + n, 4)

    peer = dev(x, y, z, 1 - k)
    sends = []

    def copy(src, dst, ssem, rsem, device):
        return pltpu.make_async_remote_copy(
            src_ref=src, dst_ref=dst, send_sem=ssem, recv_sem=rsem, device_id=device, device_id_type=MESH
        )

    free = list(range(POOL))

    def send(src, dst, rsem, device, cond=None):
        ssem = free.pop(0)

        def go():
            copy(src, dst, pool.at[ssem], rsem, device).start()

        if cond is None:
            go()
        else:
            pl.when(cond)(go)
        sends.append((src, dst, ssem, rsem, device, cond))

    def recv(dst, rsem, cond=None):
        def go():
            copy(dst, dst, pool.at[0], rsem, peer).wait_recv()

        if cond is None:
            go()
        else:
            pl.when(cond)(go)

    def ref_of(stage, color, phase, where, half):
        name, c0, cn, rows = STAGES[stage]
        buf = bufs[name]
        r0, rn, rh = rows[color]
        cols = pl.ds(c0, cn)
        rr = pl.ds(r0, rn)
        parts = {None: rr, 0: pl.ds(r0, rh), 1: pl.ds(r0 + rh, rn - rh)}
        two = {None: slice(None), 0: pl.ds(0, 2), 1: pl.ds(2, 2)}
        one = {None: slice(None), 0: pl.ds(0, 1), 1: pl.ds(1, 1)}
        axis = ORDERS[color][phase]
        if phase == 0:
            if axis == "x":
                return buf.at[where, z, y, parts[half], cols]
            if axis == "y":
                return buf.at[xi0, z, where, parts[half], cols]
            return buf.at[xi0, where, y, parts[half], cols]
        if color == 0:
            if axis == "y":
                return buf.at[one[half], z, where, rr, cols]
            return buf.at[one[half], where, :, rr, cols]
        if color == 1:
            if axis == "z":
                return buf.at[xi0, where, two[half], rr, cols]
            return buf.at[where, two[half], :, rr, cols]
        if axis == "x":
            return buf.at[where, two[half], y, rr, cols]
        return buf.at[one[half], :, where, rr, cols]

    slots = {}

    def first_slot(stage, color):
        return slots[stage, color, 0, 0]

    def context(stage, color, phase):
        axis = ORDERS[color][phase]
        rs = [ag_recv.at[slots.setdefault((stage, color, phase, i), len(slots))] for i in SLOTS[phase > 0, axis == "x"]]
        only_sources = is_source if ORDERS[color].index("x") > phase else None
        return axis, rs, only_sources

    def ring(axis):
        if axis == "y":
            return y, dev(x, up(y), z, k), dev(x, up(y, 3), z, k)
        return z, dev(x, y, up(z), k), dev(x, y, up(z, 3), k)

    def start1(stage, color, phase):
        axis, rs, cond = context(stage, color, phase)
        if axis == "x":
            if phase == 0:
                r = ref_of(stage, color, phase, xi0, None)
                for d in (1, 3, 2):
                    send(r, r, ag_recv.at[first_slot(stage, color) + xi0], dev(up(x, d), y, z, k), is_source)
                return
            inward = dev(jnp.where(pos == 0, up(x), up(x, 3)), y, z, k)
            outward = dev(jnp.where(pos == 0, up(x, 3), up(x)), y, z, k)
            h0, h1 = (ref_of(stage, color, phase, xi0, h) for h in (0, 1))
            send(h0, h0, rs[0], inward, is_source)
            send(h1, h1, rs[0], outward, is_source)
            send(h1, h1, rs[1], inward, is_source)
            send(h0, h0, rs[1], outward, is_source)
        else:
            at, right, left = ring(axis)
            if phase == 0:
                r = ref_of(stage, color, phase, at, None)
                send(r, r, rs[0], right, cond)
                send(r, r, rs[1], left, cond)
                across = dev(x, up(y, 2), z, k) if axis == "y" else dev(x, y, up(z, 2), k)
                send(r, r, rs[2], across, cond)
                return
            h0, h1 = (ref_of(stage, color, phase, at, h) for h in (0, 1))
            send(h0, h0, rs[0], right, cond)
            send(h1, h1, rs[1], left, cond)
            send(h1, h1, rs[2], right, cond)
            send(h0, h0, rs[3], left, cond)

    def turn(stage, color, phase):
        axis, rs, cond = context(stage, color, phase)
        if axis == "x":
            other = 1 - xi0
            h0, h1 = (ref_of(stage, color, phase, other, h) for h in (0, 1))
            to_low = dev(jnp.where(pos == 0, up(x, 3), up(x)), y, z, k)
            to_high = dev(jnp.where(pos == 2, up(x), up(x, 3)), y, z, k)
            recv(h0, rs[0], pos < 2)
            recv(h1, rs[0], pos >= 2)
            send(h0, h0, rs[2], to_low, pos < 2)
            send(h1, h1, rs[3], to_high, pos >= 2)
        else:
            at, right, left = ring(axis)
            h0 = ref_of(stage, color, phase, up(at, 3), 0)
            h1 = ref_of(stage, color, phase, up(at), 1)
            recv(h0, rs[0], cond)
            send(h0, h0, rs[4], right, cond)
            recv(h1, rs[1], cond)
            send(h1, h1, rs[5], left, cond)

    def finish(stage, color, phase):
        axis, rs, cond = context(stage, color, phase)
        if axis == "x":
            other = 1 - xi0
            if phase == 0:
                base = first_slot(stage, color)
                recv(ref_of(stage, color, phase, other, None), ag_recv.at[base + other])
                recv(ref_of(stage, color, phase, xi0, None), ag_recv.at[base + xi0], pos >= 2)
                return
            recv(ref_of(stage, color, phase, other, 1), rs[1], pos < 2)
            recv(ref_of(stage, color, phase, other, 0), rs[1], pos >= 2)
            recv(ref_of(stage, color, phase, xi0, 0), rs[2], pos >= 2)
            recv(ref_of(stage, color, phase, xi0, 1), rs[3], pos >= 2)
        else:
            at, _, _ = ring(axis)
            if phase == 0:
                for d, i in ((3, 0), (1, 1), (2, 2)):
                    recv(ref_of(stage, color, phase, up(at, d), None), rs[i], cond)
                return
            recv(ref_of(stage, color, phase, up(at, 3), 1), rs[2], cond)
            recv(ref_of(stage, color, phase, up(at), 0), rs[3], cond)
            recv(ref_of(stage, color, phase, up(at, 2), 0), rs[4], cond)
            recv(ref_of(stage, color, phase, up(at, 2), 1), rs[5], cond)

    def all_colors(step, stage, phase):
        for color in range(3):
            step(stage, color, phase)

    def flush(count=None):
        for _ in range(len(sends) if count is None else count):
            src, dst, ssem, rsem, device, cond = sends.pop(0)

            def done():
                copy(src, dst, pool.at[ssem], rsem, device).wait_send()

            if cond is None:
                done()
            else:
                pl.when(cond)(done)
            free.append(ssem)

    own_rows = pl.ds(pl.multiple_of(k * 64, 64), 64)
    barrier = pltpu.get_barrier_semaphore()
    y_up, z_up = up(y), up(z)
    partners = [
        peer, dev(up(x), y, z, k), dev(up(x, 3), y, z, k),
        dev(x, y_up, z, k), dev(x, up(y, 3), z, k), dev(x, y, z_up, k), dev(x, y, up(z, 3), k),
        dev(up(x, 2), y, z, k), dev(x, up(y, 2), z, k), dev(x, y, up(z, 2), k),
    ]
    for partner in partners:
        pl.semaphore_signal(barrier, inc=1, device_id=partner, device_id_type=MESH)
    own = pl.multiple_of(x * 256, 256)
    local = pltpu.make_async_copy(tokens.at[pl.ds(own, 256), :], x_buf.at[k, x], loc_sem)
    local.start()
    for load in loads:
        load.wait()
    shard = jnp.concatenate([wcv[...], wcg[...], wq[...], wk[...], wv[...]], axis=1)

    @pl.when(is_source)
    def _():
        w[xi0, z, y, own_rows, :] = shard

    @pl.when(jnp.logical_not(is_source))
    def _():
        mine_w[...] = shard

    mine_p[...] = jnp.concatenate([attn_proj[...], conv_proj[...]], axis=0)
    small[xi0, 0:31, :] = taps[...]
    small[xi0, 31:32, :] = conv_gain[...]
    small[xi0, 32:33, :] = jnp.concatenate(
        [jnp.broadcast_to(sinks[:, h : h + 1], (1, 64)) for h in range(4)], axis=1
    )

    pl.semaphore_wait(barrier, len(partners))

    not_source = jnp.logical_not(is_source)
    slot = w.at[xi0, z, y, own_rows, :]
    send(mine_w, slot, d2d_recv.at[0], peer, not_source)
    send(mine_p, peer_p, d2d_recv.at[1], peer)
    peer_rows = pl.ds(pl.multiple_of((1 - k) * 64, 64), 64)
    recv(w.at[xi0, z, y, peer_rows, :], d2d_recv.at[0], is_source)
    all_colors(start1, 0, 0)
    all_colors(start1, 1, 0)

    right, left, across = dev(up(x), y, z, k), dev(up(x, 3), y, z, k), up(x, 2)

    def token_sends(far):
        for to, device, i in ((up(x), right, 0), (up(x, 3), left, 1)):
            if far:
                block = tokens.at[pl.ds(pl.multiple_of(across * 256 + i * 128, 128), 128), :]
                send(block, hop.at[i], hop_recv.at[i], device)
            else:
                block = tokens.at[pl.ds(pl.multiple_of(to * 256, 256), 256), :]
                send(block, x_buf.at[k, x], tok_recv.at[i], device)

    def token_hops():
        for origin, device, i in ((up(x, 3), right, 0), (up(x), left, 1)):
            recv(hop.at[i], hop_recv.at[i])
            send(hop.at[i], x_buf.at[k, origin, pl.ds(i * 128, 128), :], tok_recv.at[2 + i], device)

    def tokens_on():
        for i, origin in ((0, up(x, 3)), (1, up(x))):
            recv(x_buf.at[k, origin], tok_recv.at[i])
            send(x_buf.at[k, origin], x_buf.at[k, origin], fwd_recv.at[1 + i], peer)
        for i in (0, 1):
            recv(x_buf.at[k, across, pl.ds(i * 128, 128), :], tok_recv.at[2 + i])
        send(x_buf.at[k, across], x_buf.at[k, across], fwd_recv.at[3], peer)

    def small_on():
        recv(small.at[1 - xi0], sm_recv.at[1 - xi0])
        beyond = dev(jnp.where(jnp.logical_or(pos == 0, pos == 3), up(x, 3), up(x)), y, z, k)
        send(small.at[1 - xi0], small.at[1 - xi0], sm_recv.at[1 - xi0], beyond, is_source)

    token_sends(True)
    recv(peer_p, d2d_recv.at[1])

    @pl.when(is_source)
    def _():
        a, b = mine_p[...], peer_p[...]
        low = jnp.where(k == 0, a, b)
        high = jnp.where(k == 0, b, a)
        p[xi0, z, y, 0:256, :] = jnp.concatenate([low[:64], high[:64]], axis=0).T
        p[xi0, z, y, 256:512, :] = jnp.concatenate([low[64:], high[64:]], axis=0).T

    all_colors(start1, 2, 0)
    token_sends(False)
    send(tokens.at[pl.ds(own, 256), :], x_buf.at[k, x], fwd_recv.at[0], peer)
    mine_small = small.at[xi0]
    for i, device in enumerate((right, left)):
        send(mine_small, mine_small, sm_recv.at[xi0], device, is_source)
    all_colors(finish, 0, 0)
    initial = len(sends)
    all_colors(start1, 0, 1)
    all_colors(finish, 1, 0)
    all_colors(start1, 1, 1)
    all_colors(finish, 2, 0)
    token_hops()
    all_colors(turn, 0, 1)
    all_colors(start1, 2, 1)
    all_colors(turn, 1, 1)
    all_colors(finish, 0, 1)
    early = len(sends) - initial
    all_colors(start1, 0, 2)
    all_colors(turn, 2, 1)
    all_colors(finish, 1, 1)
    flush(initial)
    small_on()
    tokens_on()
    all_colors(turn, 0, 2)
    all_colors(start1, 1, 2)
    local.wait()
    recv(x_buf.at[1 - k, x], fwd_recv.at[0])
    for i, origin in ((1, up(x, 3)), (2, up(x)), (3, across)):
        recv(x_buf.at[1 - k, origin], fwd_recv.at[i])

    def norm_rows(i, _):
        s, r = i // 8, lax.rem(i, 8)
        rows = pl.ds(pl.multiple_of(r * 32, 32), 32)
        parts = [x_buf[s, f, rows, :].astype(F32) for f in range(4)]
        square = sum(jnp.sum(v * v, axis=-1, keepdims=True) for v in parts)
        scale = lax.rsqrt(square * (1.0 / 2048) + EPSILON)
        for f in range(4):
            normed[pl.ds(pl.multiple_of(i * 32, 32), 32), f * 512 : f * 512 + 512] = (
                parts[f] * scale * mix_gain[:, f * 512 : f * 512 + 512]
            ).astype(BF)
        return 0

    lax.fori_loop(0, 16, norm_rows, 0)

    flush(early)
    middle = len(sends)
    all_colors(finish, 2, 1)
    all_colors(finish, 0, 2)

    lane = lax.broadcasted_iota(jnp.int32, (256, 128), 1)
    low_lane = lane < 64
    key_row = jnp.concatenate([key_gain[...], jnp.ones_like(key_gain[...])], axis=1)
    query_row = jnp.concatenate([query_gain[...], query_gain[...]], axis=1)

    def project(s, xi, cols):
        lhs = normed[pl.ds(pl.multiple_of(s * 256, 256), 256), :]
        rhs = w[xi, :, :, :, cols[0] : cols[1]].reshape(2048, cols[1] - cols[0])
        return jnp.dot(lhs, rhs, preferred_element_type=F32)

    def gated_part(i, _):
        xi, s = i // 2, lax.rem(i, 2)
        both = project(s, xi, (0, 512))
        value, gate = both[:, :256], both[:, 256:]
        rounded = (value * jax.nn.sigmoid(gate)).astype(BF)
        gated = rounded.astype(F32)
        for half in (0, 1):
            lanes = slice(half * 128, half * 128 + 128)
            ge[s, xi * 2 + half, 16:272, :] = gated[:, lanes]
            edge_send[s, 0, xi * 2 + half] = rounded[240:, lanes]
            edge_send[s, 1, xi * 2 + half] = rounded[:16, lanes]
        return 0

    lax.fori_loop(0, 4, gated_part, 0)

    def neighbour(s, side):
        wraps, over = (x == 3, 1) if side == 0 else (x == 0, 15)
        step = jnp.where(jnp.logical_and(wraps, s == 1 - side), over, 0)
        return (lax.rem(q + step, 16) * 2 + k, up(x, 1 if side == 0 else 3)), jnp.where(wraps, 1 - s, s)

    SIDES = ((0, 0), (0, 1), (1, 0), (1, 1))
    is_first = jnp.logical_and(q == 0, x == 0)
    is_last = jnp.logical_and(q == 15, x == 3)

    for s, side in SIDES:
        to, seg = neighbour(s, side)
        send(edge_send.at[s, side], edge_recv.at[seg, side],
             halo_recv.at[4 + seg * 2 + side], to)
    all_colors(turn, 1, 2)
    all_colors(start1, 2, 2)
    recv(small.at[xi0], sm_recv.at[xi0], not_source)
    for s, side in SIDES:
        recv(edge_recv.at[s, side], halo_recv.at[4 + s * 2 + side])
        ge[s, :, side * 272 : side * 272 + 16, :] = edge_recv[s, side].astype(F32)

    @pl.when(is_first)
    def _():
        ge[0, :, 0:16, :] = jnp.zeros((4, 16, 128), F32)

    @pl.when(is_last)
    def _():
        ge[1, :, 272:288, :] = jnp.zeros((4, 16, 128), F32)

    def conv_block(i, _):
        s, cb = i // 4, lax.rem(i, 4)
        xi, half = cb // 2, lax.rem(cb, 2)
        tap_rows = jnp.where(half == 0, small[xi, :, 0:128], small[xi, :, 128:256])
        for r in (0, 128):
            total = jnp.zeros((128, 128), F32)
            for t in range(31):
                total = total + tap_rows[t : t + 1, :] * ge[s, cb, r + 1 + t : r + 129 + t, :]
            conv[cb, pl.ds(pl.multiple_of(s * 256, 256) + r, 128), :] = total
        return 0

    lax.fori_loop(0, 8, conv_block, 0)

    all_colors(finish, 1, 2)

    def project_both(s, cols):
        lhs = normed[pl.ds(pl.multiple_of(s * 256, 256), 256), :]
        width = cols[1] - cols[0]
        rhs = jnp.concatenate([w[xi, :, :, :, cols[0] : cols[1]].reshape(2048, width) for xi in (0, 1)], axis=1)
        both = jnp.dot(lhs, rhs, preferred_element_type=F32)
        return both[:, :width], both[:, width:]

    def first_part(s, _):
        for xi, kv in enumerate(project_both(s, KV)):
            square = jnp.sum(jnp.where(low_lane, kv * kv, 0.0), axis=-1, keepdims=True)
            keyed = kv * lax.rsqrt(square * (1.0 / 64) + EPSILON) * key_row
            kve[s, xi, 128:384, :] = jnp.where(low_lane, keyed, kv).astype(BF)
        return 0

    lax.fori_loop(0, 2, first_part, 0)
    for s, side in SIDES:
        to, seg = neighbour(s, side)
        src, dst = (256, 0) if side == 0 else (128, 384)
        send(kve.at[s, :, pl.ds(src, 128), :], kve.at[seg, :, pl.ds(dst, 128), :], halo_recv.at[seg * 2 + side], to)
    def stats(i, _):
        rows = pl.ds(pl.multiple_of(i * 64, 64), 64)
        blocks = [conv[cb, rows, :] for cb in range(4)]
        mean = jnp.sum(blocks[0] + blocks[1] + blocks[2] + blocks[3], axis=-1, keepdims=True) * (1.0 / 512)
        dev_sq = sum((b - mean) * (b - mean) for b in blocks)
        m2 = jnp.sum(dev_sq, axis=-1, keepdims=True)
        stat_own[rows, :] = jnp.where(low_lane[:64], mean, m2)
        return 0

    lax.fori_loop(0, 8, stats, 0)
    send(stat_own, stat_peer, stat_recv.at[0], peer)

    def query_part(s, _):
        for xi, full in enumerate(project_both(s, Q)):
            for pair in (0, 1):
                v = full[:, pair * 128 : pair * 128 + 128]
                sq = v * v
                even = jnp.sum(jnp.where(low_lane, sq, 0.0), axis=-1, keepdims=True)
                odd = jnp.sum(jnp.where(low_lane, 0.0, sq), axis=-1, keepdims=True)
                scale = lax.rsqrt(jnp.where(low_lane, even, odd) * (1.0 / 64) + EPSILON)
                rounded = (v * scale * query_row).astype(BF).astype(F32) * 0.125
                qn[xi * 2 + pair, pl.ds(pl.multiple_of(s * 256, 256), 256), :] = rounded.astype(BF)
        return 0

    lax.fori_loop(0, 2, query_part, 0)
    recv(stat_peer, stat_recv.at[0])

    def feature(i, _):
        rows = pl.ds(pl.multiple_of(i * 64, 64), 64)
        a, b = stat_own[rows, :], stat_peer[rows, :]
        mean = 0.5 * (a[:, 0:1] + b[:, 0:1])
        gap = a[:, 0:1] - b[:, 0:1]
        spread = (a[:, 64:65] + b[:, 64:65] + gap * gap * 256.0) * (1.0 / 1024)
        scale = lax.rsqrt(spread + EPSILON)
        for cb in range(4):
            xi, half = cb // 2, cb % 2
            gain = small[xi, 31:32, half * 128 : half * 128 + 128]
            v = (conv[cb, rows, :] - mean) * scale * gain
            feats[rows, xi * 512 + 256 + half * 128 : xi * 512 + 384 + half * 128] = (v * jax.nn.sigmoid(v)).astype(BF)
        return 0

    lax.fori_loop(0, 8, feature, 0)
    all_colors(turn, 2, 2)
    flush(middle)
    row_i = lax.rem(lax.broadcasted_iota(jnp.int32, (256, 384), 0), 128)
    col_i = lax.broadcasted_iota(jnp.int32, (256, 384), 1)
    lane384 = lax.broadcasted_iota(jnp.int32, (384, 128), 1) < 64

    def attention(i):
        s, b = i // 2, i % 2
        base = s * 256 + b * 128
        first = jnp.where(jnp.logical_and(is_first, s == 0), 128, 0) - b * 128
        end = jnp.where(jnp.logical_and(is_last, s == 1), 384, 512) - b * 128
        reach = col_i - row_i
        allowed = (reach >= 0) & (reach <= 256) & (col_i >= first) & (col_i < end)
        nt = (((1,), (1,)), ((), ()))

        def mix(heads, keys, values):
            scores = lax.dot_general(heads, keys.astype(BF), nt, preferred_element_type=F32)
            weights = jnp.where(allowed, jnp.exp(scores), 0.0).astype(BF)
            return jnp.dot(weights, values.astype(BF), preferred_element_type=F32)

        for xi in (0, 1):
            kv = kve[s, xi, b * 128 : b * 128 + 384, :].astype(F32)
            swapped = pltpu.roll(kv, 64, 1)
            both = jnp.concatenate([qn[xi * 2 + pair, pl.ds(base, 128), :] for pair in (0, 1)], axis=0).astype(F32)
            even = jnp.where(low_lane, both, 0.0).astype(BF)
            odd = jnp.where(low_lane, 0.0, both).astype(BF)
            o_even = mix(even, kv, jnp.where(lane384, swapped, 1.0))
            o_odd = mix(odd, swapped, jnp.where(lane384, 1.0, kv))
            number = jnp.where(low_lane, o_even, o_odd)
            weight = pltpu.roll(jnp.where(low_lane, o_odd, o_even), 64, 1)
            sink = jnp.exp(small[xi, 32:33, :])
            for pair in (0, 1):
                rows, lanes = slice(pair * 128, pair * 128 + 128), slice(pair * 128, pair * 128 + 128)
                col = xi * 512 + pair * 128
                feats[pl.ds(base, 128), col : col + 128] = (number[rows] / (weight[rows] + sink[:, lanes])).astype(BF)

    for s, b in SIDES:
        recv(kve.at[s, :, pl.ds(b * 384, 128), :], halo_recv.at[s * 2 + b])
        attention(s * 2 + b)

    all_colors(finish, 2, 2)

    for nb in range(4):
        rhs = jnp.concatenate(
            [jnp.concatenate([p[xi, nb, yy] for yy in range(4)], axis=1) for xi in (0, 1)], axis=0
        )
        part = jnp.dot(feats[...], rhs, preferred_element_type=F32).reshape(2, 256, 512)
        part_send[nb] = part.astype(BF)
        send(part_send.at[nb, 1 - k], part_recv.at[nb], out_recv.at[nb], peer)
        part_own[nb] = part
    for nb in range(4):
        recv(part_recv.at[nb], out_recv.at[nb])
        out[:, nb * 512 : nb * 512 + 512] = (part_own[nb, k] + part_recv[nb].astype(F32)).astype(BF)
    flush()


def on_device(tokens, mix_gain, wq, wk, wv, wcv, wcg, query_gain, key_gain, sinks, taps, conv_gain, attn_proj, conv_proj):
    vmem = pl.BlockSpec(memory_space=pltpu.VMEM)
    dma = pltpu.SemaphoreType.DMA
    arrays = (
        tokens, mix_gain.reshape(1, -1), wq, wk, wv, wcv, wcg, query_gain.reshape(1, -1), key_gain.reshape(1, -1),
        sinks.reshape(1, -1), taps, conv_gain.reshape(1, -1), attn_proj.T, conv_proj.T,
    )
    return pl.pallas_call(
        kernel,
        out_shape=jax.ShapeDtypeStruct((256, 2048), BF),
        in_specs=[pl.BlockSpec(memory_space=pltpu.HBM)] * 14,
        out_specs=vmem,
        scratch_shapes=[
            *(pltpu.VMEM(a.shape, a.dtype) for a in arrays[1:]),
            pltpu.VMEM((2, 4, 4, 128, 896), BF),
            pltpu.VMEM((2, 4, 4, 512, 128), BF),
            pltpu.VMEM((64, 896), BF),
            pltpu.VMEM((128, 256), BF),
            pltpu.VMEM((128, 256), BF),
            pltpu.VMEM((2, 40, 256), F32),
            pltpu.VMEM((2, 128, 512), BF),
            pltpu.VMEM((2, 2, 4, 16, 128), BF),
            pltpu.VMEM((2, 2, 4, 16, 128), BF),
            pltpu.VMEM((2, 4, 256, 512), BF),
            pltpu.VMEM((512, 2048), BF),
            pltpu.VMEM((4, 512, 128), BF),
            pltpu.VMEM((2, 2, 512, 128), BF),
            pltpu.VMEM((2, 4, 288, 128), F32),
            pltpu.VMEM((4, 512, 128), F32),
            pltpu.VMEM((512, 128), F32),
            pltpu.VMEM((512, 128), F32),
            pltpu.VMEM((512, 1024), BF),
            pltpu.VMEM((4, 2, 256, 512), F32),
            pltpu.VMEM((4, 2, 256, 512), BF),
            pltpu.VMEM((4, 256, 512), BF),
            dma((13,)), dma((POOL,)), dma((SLOT_COUNT,)), dma((2,)), dma((4,)), dma((2,)), dma((4,)), dma(()), dma((2,)),
            dma((8,)), dma((1,)), dma((4,)),
        ],
        compiler_params=pltpu.CompilerParams(
            collective_id=0, has_side_effects=True, vmem_limit_bytes=44 * 1024 * 1024
        ),
        name="layer",
    )(*(pltpu.with_memory_space_constraint(a, pltpu.HBM) for a in arrays))


def solution(mesh):
    placed = (
        P("sp", "tp"), P(), P("sp", "tp"), P("sp", "tp"), P("sp", "tp"), P("sp", "tp"), P("sp", "tp"),
        P(), P(), P("tp"), P(None, "tp"), P("tp"), P("tp", "sp"), P("tp", "sp"),
    )
    return jax.shard_map(
        on_device, mesh=mesh, in_specs=placed, out_specs=P(("sp", "tp"), None), check_vma=False
    )
```

```python
import jax
import jax.numpy as jnp
from jax import lax
from jax.experimental import pallas as pl
from jax.experimental.pallas import tpu as pltpu
from jax.sharding import PartitionSpec as P

MESH = pl.DeviceIdType.MESH
EPSILON = 0.1
BF = jnp.bfloat16
F32 = jnp.float32

CV, CG, Q, KV = (0, 256), (256, 512), (512, 768), (768, 896)
STAGES = (
    ("w", 0, 512, ((0, 64, 32), (64, 16, 16), (80, 48, 32))),
    ("w", 512, 384, ((0, 48, 32), (48, 16, 16), (64, 64, 32))),
    ("p", 0, 128, ((0, 160, 80), (160, 192, 96), (352, 160, 80))),
)
ORDERS = ("xyz", "yzx", "zxy")
SLOTS = {(False, True): range(2), (False, False): range(3), (True, True): range(4), (True, False): range(6)}
SLOT_COUNT = 3 * sum(
    len(SLOTS[phase > 0, axis == "x"]) for order in ORDERS for phase, axis in enumerate(order)
)
POOL = 112


def kernel(
    tokens, *rest,
):
    given, (out, *held), rest = rest[:13], rest[13:27], rest[27:]
    mix_gain, wq, wk, wv, wcv, wcg, query_gain, key_gain, sinks, taps, conv_gain, attn_proj, conv_proj = held
    (
        w, p, mine_w, mine_p, peer_p, small, hop, edge_send, edge_recv, x_buf, normed, qn, kve, ge, conv, stat_own,
        stat_peer, feats, part_own, part_send, part_recv,
        load_sem, pool, ag_recv, d2d_recv, tok_recv, hop_recv, fwd_recv, loc_sem, sm_recv, halo_recv, stat_recv,
        out_recv,
    ) = rest
    loads = [pltpu.make_async_copy(a, b, load_sem.at[i]) for i, (a, b) in enumerate(zip(given, held))]
    for load in loads:
        load.start()
    sp, x = lax.axis_index("sp"), lax.axis_index("tp")
    k = lax.rem(sp, 2)
    q = sp // 2
    y, z = lax.rem(q, 4), q // 4
    pos = lax.rem(x + 4 - 2 * k, 4)
    xi0 = lax.rem(x, 2)
    is_source = pos < 2
    bufs = {"w": w, "p": p}

    def dev(xx, yy, zz, kk):
        return (zz * 8 + yy * 2 + kk, xx)

    def up(v, n=1):
        return lax.rem(v + n, 4)

    peer = dev(x, y, z, 1 - k)
    sends = []

    def copy(src, dst, ssem, rsem, device):
        return pltpu.make_async_remote_copy(
            src_ref=src, dst_ref=dst, send_sem=ssem, recv_sem=rsem, device_id=device, device_id_type=MESH
        )

    free = list(range(POOL))

    def send(src, dst, rsem, device, cond=None):
        ssem = free.pop(0)

        def go():
            copy(src, dst, pool.at[ssem], rsem, device).start()

        if cond is None:
            go()
        else:
            pl.when(cond)(go)
        sends.append((src, dst, ssem, rsem, device, cond))

    def recv(dst, rsem, cond=None):
        def go():
            copy(dst, dst, pool.at[0], rsem, peer).wait_recv()

        if cond is None:
            go()
        else:
            pl.when(cond)(go)

    def ref_of(stage, color, phase, where, half):
        name, c0, cn, rows = STAGES[stage]
        buf = bufs[name]
        r0, rn, rh = rows[color]
        cols = pl.ds(c0, cn)
        rr = pl.ds(r0, rn)
        two = {None: slice(None), 0: pl.ds(0, 2), 1: pl.ds(2, 2)}
        one = {None: slice(None), 0: pl.ds(0, 1), 1: pl.ds(1, 1)}
        axis = ORDERS[color][phase]
        if phase == 0:
            if axis == "x":
                return buf.at[where, z, y, rr, cols]
            if axis == "y":
                return buf.at[xi0, z, where, rr, cols]
            return buf.at[xi0, where, y, rr, cols]
        if color == 0:
            if axis == "y":
                return buf.at[one[half], z, where, rr, cols]
            return buf.at[one[half], where, :, rr, cols]
        if color == 1:
            if axis == "z":
                return buf.at[xi0, where, two[half], rr, cols]
            return buf.at[where, two[half], :, rr, cols]
        if axis == "x":
            return buf.at[where, two[half], y, rr, cols]
        return buf.at[one[half], :, where, rr, cols]

    slots = {}

    def first_slot(stage, color):
        return slots[stage, color, 0, 0]

    def context(stage, color, phase):
        axis = ORDERS[color][phase]
        rs = [ag_recv.at[slots.setdefault((stage, color, phase, i), len(slots))] for i in SLOTS[phase > 0, axis == "x"]]
        only_sources = is_source if ORDERS[color].index("x") > phase else None
        return axis, rs, only_sources

    def ring(axis):
        if axis == "y":
            return y, dev(x, up(y), z, k), dev(x, up(y, 3), z, k)
        return z, dev(x, y, up(z), k), dev(x, y, up(z, 3), k)

    def start1(stage, color, phase):
        axis, rs, cond = context(stage, color, phase)
        if axis == "x":
            if phase == 0:
                r = ref_of(stage, color, phase, xi0, None)
                for d in (1, 3, 2):
                    send(r, r, ag_recv.at[first_slot(stage, color) + xi0], dev(up(x, d), y, z, k), is_source)
                return
            inward = dev(jnp.where(pos == 0, up(x), up(x, 3)), y, z, k)
            outward = dev(jnp.where(pos == 0, up(x, 3), up(x)), y, z, k)
            h0, h1 = (ref_of(stage, color, phase, xi0, h) for h in (0, 1))
            send(h0, h0, rs[0], inward, is_source)
            send(h1, h1, rs[0], outward, is_source)
            send(h1, h1, rs[1], inward, is_source)
            send(h0, h0, rs[1], outward, is_source)
        else:
            at, right, left = ring(axis)
            if phase == 0:
                r = ref_of(stage, color, phase, at, None)
                send(r, r, rs[0], right, cond)
                send(r, r, rs[1], left, cond)
                across = dev(x, up(y, 2), z, k) if axis == "y" else dev(x, y, up(z, 2), k)
                send(r, r, rs[2], across, cond)
                return
            h0, h1 = (ref_of(stage, color, phase, at, h) for h in (0, 1))
            send(h0, h0, rs[0], right, cond)
            send(h1, h1, rs[1], left, cond)
            send(h1, h1, rs[2], right, cond)
            send(h0, h0, rs[3], left, cond)

    def turn(stage, color, phase):
        axis, rs, cond = context(stage, color, phase)
        if axis == "x":
            other = 1 - xi0
            h0, h1 = (ref_of(stage, color, phase, other, h) for h in (0, 1))
            to_low = dev(jnp.where(pos == 0, up(x, 3), up(x)), y, z, k)
            to_high = dev(jnp.where(pos == 2, up(x), up(x, 3)), y, z, k)
            recv(h0, rs[0], pos < 2)
            recv(h1, rs[0], pos >= 2)
            send(h0, h0, rs[2], to_low, pos < 2)
            send(h1, h1, rs[3], to_high, pos >= 2)
        else:
            at, right, left = ring(axis)
            h0 = ref_of(stage, color, phase, up(at, 3), 0)
            h1 = ref_of(stage, color, phase, up(at), 1)
            recv(h0, rs[0], cond)
            send(h0, h0, rs[4], right, cond)
            recv(h1, rs[1], cond)
            send(h1, h1, rs[5], left, cond)

    def finish(stage, color, phase):
        axis, rs, cond = context(stage, color, phase)
        if axis == "x":
            other = 1 - xi0
            if phase == 0:
                base = first_slot(stage, color)
                recv(ref_of(stage, color, phase, other, None), ag_recv.at[base + other])
                recv(ref_of(stage, color, phase, xi0, None), ag_recv.at[base + xi0], pos >= 2)
                return
            recv(ref_of(stage, color, phase, other, 1), rs[1], pos < 2)
            recv(ref_of(stage, color, phase, other, 0), rs[1], pos >= 2)
            recv(ref_of(stage, color, phase, xi0, 0), rs[2], pos >= 2)
            recv(ref_of(stage, color, phase, xi0, 1), rs[3], pos >= 2)
        else:
            at, _, _ = ring(axis)
            if phase == 0:
                for d, i in ((3, 0), (1, 1), (2, 2)):
                    recv(ref_of(stage, color, phase, up(at, d), None), rs[i], cond)
                return
            recv(ref_of(stage, color, phase, up(at, 3), 1), rs[2], cond)
            recv(ref_of(stage, color, phase, up(at), 0), rs[3], cond)
            recv(ref_of(stage, color, phase, up(at, 2), 0), rs[4], cond)
            recv(ref_of(stage, color, phase, up(at, 2), 1), rs[5], cond)

    def all_colors(step, stage, phase):
        for color in range(3):
            step(stage, color, phase)

    def flush(count=None):
        for _ in range(len(sends) if count is None else count):
            src, dst, ssem, rsem, device, cond = sends.pop(0)

            def done():
                copy(src, dst, pool.at[ssem], rsem, device).wait_send()

            if cond is None:
                done()
            else:
                pl.when(cond)(done)
            free.append(ssem)

    own_rows = pl.ds(pl.multiple_of(k * 64, 64), 64)
    barrier = pltpu.get_barrier_semaphore()
    y_up, z_up = up(y), up(z)
    partners = [
        peer, dev(up(x), y, z, k), dev(up(x, 3), y, z, k),
        dev(x, y_up, z, k), dev(x, up(y, 3), z, k), dev(x, y, z_up, k), dev(x, y, up(z, 3), k),
        dev(up(x, 2), y, z, k), dev(x, up(y, 2), z, k), dev(x, y, up(z, 2), k),
    ]
    for partner in partners:
        pl.semaphore_signal(barrier, inc=1, device_id=partner, device_id_type=MESH)
    own = pl.multiple_of(x * 256, 256)
    local = pltpu.make_async_copy(tokens.at[pl.ds(own, 256), :], x_buf.at[k, x], loc_sem)
    local.start()
    for load in loads:
        load.wait()
    shard = jnp.concatenate([wcv[...], wcg[...], wq[...], wk[...], wv[...]], axis=1)

    @pl.when(is_source)
    def _():
        w[xi0, z, y, own_rows, :] = shard

    @pl.when(jnp.logical_not(is_source))
    def _():
        mine_w[...] = shard

    mine_p[...] = jnp.concatenate([attn_proj[...], conv_proj[...]], axis=0)
    small[xi0, 0:31, :] = taps[...]
    small[xi0, 31:32, :] = conv_gain[...]
    small[xi0, 32:33, :] = jnp.concatenate(
        [jnp.broadcast_to(sinks[:, h : h + 1], (1, 64)) for h in range(4)], axis=1
    )

    pl.semaphore_wait(barrier, len(partners))

    not_source = jnp.logical_not(is_source)
    slot = w.at[xi0, z, y, own_rows, :]
    send(mine_w, slot, d2d_recv.at[0], peer, not_source)
    send(mine_p, peer_p, d2d_recv.at[1], peer)
    peer_rows = pl.ds(pl.multiple_of((1 - k) * 64, 64), 64)
    recv(w.at[xi0, z, y, peer_rows, :], d2d_recv.at[0], is_source)
    all_colors(start1, 0, 0)
    all_colors(start1, 1, 0)

    right, left, across = dev(up(x), y, z, k), dev(up(x, 3), y, z, k), up(x, 2)

    def token_sends(far):
        for to, device, i in ((up(x), right, 0), (up(x, 3), left, 1)):
            if far:
                block = tokens.at[pl.ds(pl.multiple_of(across * 256 + i * 128, 128), 128), :]
                send(block, hop.at[i], hop_recv.at[i], device)
            else:
                block = tokens.at[pl.ds(pl.multiple_of(to * 256, 256), 256), :]
                send(block, x_buf.at[k, x], tok_recv.at[i], device)

    def token_hops():
        for origin, device, i in ((up(x, 3), right, 0), (up(x), left, 1)):
            recv(hop.at[i], hop_recv.at[i])
            send(hop.at[i], x_buf.at[k, origin, pl.ds(i * 128, 128), :], tok_recv.at[2 + i], device)

    def tokens_near():
        for i, origin in ((0, up(x, 3)), (1, up(x))):
            recv(x_buf.at[k, origin], tok_recv.at[i])
            send(x_buf.at[k, origin], x_buf.at[k, origin], fwd_recv.at[1 + i], peer)

    def tokens_far():
        for i in (0, 1):
            recv(x_buf.at[k, across, pl.ds(i * 128, 128), :], tok_recv.at[2 + i])
        send(x_buf.at[k, across], x_buf.at[k, across], fwd_recv.at[3], peer)

    def small_on():
        recv(small.at[1 - xi0], sm_recv.at[1 - xi0])
        beyond = dev(jnp.where(jnp.logical_or(pos == 0, pos == 3), up(x, 3), up(x)), y, z, k)
        send(small.at[1 - xi0], small.at[1 - xi0], sm_recv.at[1 - xi0], beyond, is_source)

    recv(peer_p, d2d_recv.at[1])

    @pl.when(is_source)
    def _():
        a, b = mine_p[...], peer_p[...]
        low = jnp.where(k == 0, a, b)
        high = jnp.where(k == 0, b, a)
        p[xi0, z, y, 0:256, :] = jnp.concatenate([low[:64], high[:64]], axis=0).T
        p[xi0, z, y, 256:512, :] = jnp.concatenate([low[64:], high[64:]], axis=0).T

    def onward(last, following):
        for color in range(3):
            finish(last[0], color, last[1])
            start1(following[0], color, following[1])

    all_colors(start1, 2, 0)
    onward((0, 0), (0, 1))
    onward((1, 0), (1, 1))
    token_sends(True)
    all_colors(finish, 2, 0)
    initial = len(sends)
    all_colors(turn, 0, 1)
    all_colors(start1, 2, 1)
    all_colors(turn, 1, 1)
    token_sends(False)
    send(tokens.at[pl.ds(own, 256), :], x_buf.at[k, x], fwd_recv.at[0], peer)
    mine_small = small.at[xi0]
    for device in (right, left):
        send(mine_small, mine_small, sm_recv.at[xi0], device, is_source)
    onward((0, 1), (0, 2))
    early = len(sends) - initial
    token_hops()
    flush(initial)
    all_colors(turn, 2, 1)
    for color in (0, 2, 1):
        turn(0, color, 2)
        finish(1, color, 1)
        start1(1, color, 2)
        if color == 2:
            tokens_near()
    tokens_far()
    small_on()
    local.wait()

    def norm_rows(s):
        def body(r, _):
            rows = pl.ds(pl.multiple_of(r * 32, 32), 32)
            parts = [x_buf[s, f, rows, :].astype(F32) for f in range(4)]
            square = sum(jnp.sum(v * v, axis=-1, keepdims=True) for v in parts)
            scale = lax.rsqrt(square * (1.0 / 2048) + EPSILON)
            for f in range(4):
                normed[pl.ds(pl.multiple_of(s * 256 + r * 32, 32), 32), f * 512 : f * 512 + 512] = (
                    parts[f] * scale * mix_gain[:, f * 512 : f * 512 + 512]
                ).astype(BF)
            return 0

        lax.fori_loop(0, 8, body, 0)

    norm_rows(k)
    recv(x_buf.at[1 - k, x], fwd_recv.at[0])
    for i, origin in ((1, up(x, 3)), (2, up(x)), (3, across)):
        recv(x_buf.at[1 - k, origin], fwd_recv.at[i])
    norm_rows(1 - k)
    flush(early)
    middle = len(sends)
    all_colors(finish, 2, 1)
    all_colors(finish, 0, 2)

    lane = lax.broadcasted_iota(jnp.int32, (256, 128), 1)
    low_lane = lane < 64
    key_row = jnp.concatenate([key_gain[...], jnp.ones_like(key_gain[...])], axis=1)
    query_row = jnp.concatenate([query_gain[...], query_gain[...]], axis=1)

    def project(s, xi, cols):
        lhs = normed[pl.ds(s * 256, 256), :]
        rhs = w[xi, :, :, :, cols[0] : cols[1]].reshape(2048, cols[1] - cols[0])
        return jnp.dot(lhs, rhs, preferred_element_type=F32)

    def gated_part(s, xi):
        both = project(s, xi, (0, 512))
        value, gate = both[:, :256], both[:, 256:]
        rounded = (value * jax.nn.sigmoid(gate)).astype(BF)
        gated = rounded.astype(F32)
        for half in (0, 1):
            lanes = slice(half * 128, half * 128 + 128)
            ge[s, xi * 2 + half, 16:272, :] = gated[:, lanes]
            edge_send[s, 0, xi * 2 + half] = rounded[240:, lanes]
            edge_send[s, 1, xi * 2 + half] = rounded[:16, lanes]

    def neighbour(s, side):
        wraps, over = (x == 3, 1) if side == 0 else (x == 0, 15)
        step = jnp.where(jnp.logical_and(wraps, s == 1 - side), over, 0)
        return (lax.rem(q + step, 16) * 2 + k, up(x, 1 if side == 0 else 3)), jnp.where(wraps, 1 - s, s)

    SIDES = ((0, 0), (0, 1), (1, 0), (1, 1))
    is_first = jnp.logical_and(q == 0, x == 0)
    is_last = jnp.logical_and(q == 15, x == 3)

    for s in (0, 1):
        for xi in (0, 1):
            gated_part(s, xi)
        for side in (0, 1):
            to, seg = neighbour(s, side)
            send(edge_send.at[s, side], edge_recv.at[seg, side], halo_recv.at[4 + seg * 2 + side], to)
    all_colors(turn, 1, 2)
    all_colors(start1, 2, 2)
    recv(small.at[xi0], sm_recv.at[xi0], not_source)
    def conv_block(segment, cb):
        xi, half = cb // 2, lax.rem(cb, 2)
        tap_rows = jnp.where(half == 0, small[xi, :, 0:128], small[xi, :, 128:256])
        for r in (0, 128):
            total = jnp.zeros((128, 128), F32)
            for t in range(31):
                total = total + tap_rows[t : t + 1, :] * ge[segment, cb, r + 1 + t : r + 129 + t, :]
            conv[cb, segment * 256 + r : segment * 256 + r + 128, :] = total

    for s in (0, 1):
        for side in (0, 1):
            recv(edge_recv.at[s, side], halo_recv.at[4 + s * 2 + side])
            ge[s, :, side * 272 : side * 272 + 16, :] = edge_recv[s, side].astype(F32)

        @pl.when(is_first if s == 0 else is_last)
        def _():
            ge[s, :, s * 272 : s * 272 + 16, :] = jnp.zeros((4, 16, 128), F32)

        def conv_step(cb, _, s=s):
            conv_block(s, cb)
            return 0

        lax.fori_loop(0, 4, conv_step, 0)

    all_colors(finish, 1, 2)

    def project_both(s, cols):
        lhs = normed[pl.ds(s * 256, 256), :]
        width = cols[1] - cols[0]
        rhs = jnp.concatenate([w[xi, :, :, :, cols[0] : cols[1]].reshape(2048, width) for xi in (0, 1)], axis=1)
        both = jnp.dot(lhs, rhs, preferred_element_type=F32)
        return both[:, :width], both[:, width:]

    def first_part(s, _):
        for xi, kv in enumerate(project_both(s, KV)):
            square = jnp.sum(jnp.where(low_lane, kv * kv, 0.0), axis=-1, keepdims=True)
            keyed = kv * lax.rsqrt(square * (1.0 / 64) + EPSILON) * key_row
            kve[s, xi, 128:384, :] = jnp.where(low_lane, keyed, kv).astype(BF)
        return 0

    for s, side in SIDES:
        if side == 0:
            first_part(s, 0)
        to, seg = neighbour(s, side)
        src, dst = (256, 0) if side == 0 else (128, 384)
        send(kve.at[s, :, pl.ds(src, 128), :], kve.at[seg, :, pl.ds(dst, 128), :], halo_recv.at[seg * 2 + side], to)
    def stats(i, _):
        rows = pl.ds(pl.multiple_of(i * 64, 64), 64)
        blocks = [conv[cb, rows, :] for cb in range(4)]
        mean = jnp.sum(blocks[0] + blocks[1] + blocks[2] + blocks[3], axis=-1, keepdims=True) * (1.0 / 512)
        dev_sq = sum((b - mean) * (b - mean) for b in blocks)
        m2 = jnp.sum(dev_sq, axis=-1, keepdims=True)
        stat_own[rows, :] = jnp.where(low_lane[:64], mean, m2)
        return 0

    lax.fori_loop(0, 8, stats, 0)
    send(stat_own, stat_peer, stat_recv.at[0], peer)

    def query_part(s, _):
        for xi, full in enumerate(project_both(s, Q)):
            for pair in (0, 1):
                v = full[:, pair * 128 : pair * 128 + 128]
                sq = v * v
                even = jnp.sum(jnp.where(low_lane, sq, 0.0), axis=-1, keepdims=True)
                odd = jnp.sum(jnp.where(low_lane, 0.0, sq), axis=-1, keepdims=True)
                scale = lax.rsqrt(jnp.where(low_lane, even, odd) * (1.0 / 64) + EPSILON)
                rounded = (v * scale * query_row).astype(BF).astype(F32) * 0.125
                qn[xi * 2 + pair, pl.ds(s * 256, 256), :] = rounded.astype(BF)
        return 0

    for s in (0, 1):
        query_part(s, 0)
    late = len(sends) - middle
    for color in (0, 2, 1):
        turn(2, color, 2)
    recv(stat_peer, stat_recv.at[0])

    def feature(i, _):
        rows = pl.ds(pl.multiple_of(i * 64, 64), 64)
        a, b = stat_own[rows, :], stat_peer[rows, :]
        mean = 0.5 * (a[:, 0:1] + b[:, 0:1])
        gap = a[:, 0:1] - b[:, 0:1]
        spread = (a[:, 64:65] + b[:, 64:65] + gap * gap * 256.0) * (1.0 / 1024)
        scale = lax.rsqrt(spread + EPSILON)
        for cb in range(4):
            xi, half = cb // 2, cb % 2
            gain = small[xi, 31:32, half * 128 : half * 128 + 128]
            v = (conv[cb, rows, :] - mean) * scale * gain
            feats[rows, xi * 512 + 256 + half * 128 : xi * 512 + 384 + half * 128] = (v * jax.nn.sigmoid(v)).astype(BF)
        return 0

    lax.fori_loop(0, 8, feature, 0)
    flush(middle)
    row_i = lax.rem(lax.broadcasted_iota(jnp.int32, (256, 384), 0), 128)
    col_i = lax.broadcasted_iota(jnp.int32, (256, 384), 1)
    lane384 = lax.broadcasted_iota(jnp.int32, (384, 128), 1) < 64

    def attention(i):
        s, b = i // 2, i % 2
        base = s * 256 + b * 128
        first = jnp.where(jnp.logical_and(is_first, s == 0), 128, 0) - b * 128
        end = jnp.where(jnp.logical_and(is_last, s == 1), 384, 512) - b * 128
        reach = col_i - row_i
        allowed = (reach >= 0) & (reach <= 256) & (col_i >= first) & (col_i < end)
        nt = (((1,), (1,)), ((), ()))

        def mix(heads, keys, values):
            scores = lax.dot_general(heads, keys.astype(BF), nt, preferred_element_type=F32)
            weights = jnp.where(allowed, jnp.exp(scores), 0.0).astype(BF)
            return jnp.dot(weights, values.astype(BF), preferred_element_type=F32)

        for xi in (0, 1):
            kv = kve[s, xi, b * 128 : b * 128 + 384, :].astype(F32)
            swapped = pltpu.roll(kv, 64, 1)
            both = jnp.concatenate([qn[xi * 2 + pair, pl.ds(base, 128), :] for pair in (0, 1)], axis=0).astype(F32)
            even = jnp.where(low_lane, both, 0.0).astype(BF)
            odd = jnp.where(low_lane, 0.0, both).astype(BF)
            o_even = mix(even, kv, jnp.where(lane384, swapped, 1.0))
            o_odd = mix(odd, swapped, jnp.where(lane384, 1.0, kv))
            number = jnp.where(low_lane, o_even, o_odd)
            weight = pltpu.roll(jnp.where(low_lane, o_odd, o_even), 64, 1)
            sink = jnp.exp(small[xi, 32:33, :])
            for pair in (0, 1):
                rows, lanes = slice(pair * 128, pair * 128 + 128), slice(pair * 128, pair * 128 + 128)
                col = xi * 512 + pair * 128
                feats[pl.ds(base, 128), col : col + 128] = (number[rows] / (weight[rows] + sink[:, lanes])).astype(BF)

    for s, b in SIDES:
        recv(kve.at[s, :, pl.ds(b * 384, 128), :], halo_recv.at[s * 2 + b])
        attention(s * 2 + b)

    flush(late)
    all_colors(finish, 2, 2)

    for nb in range(4):
        rhs = jnp.concatenate(
            [jnp.concatenate([p[xi, nb, yy] for yy in range(4)], axis=1) for xi in (0, 1)], axis=0
        )
        part = jnp.dot(feats[...], rhs, preferred_element_type=F32).reshape(2, 256, 512)
        part_send[nb] = part.astype(BF)
        send(part_send.at[nb, 1 - k], part_recv.at[nb], out_recv.at[nb], peer)
        part_own[nb] = part
    for nb in range(4):
        recv(part_recv.at[nb], out_recv.at[nb])
        out[:, nb * 512 : nb * 512 + 512] = (part_own[nb, k] + part_recv[nb].astype(F32)).astype(BF)
    flush()


def on_device(tokens, mix_gain, wq, wk, wv, wcv, wcg, query_gain, key_gain, sinks, taps, conv_gain, attn_proj, conv_proj):
    vmem = pl.BlockSpec(memory_space=pltpu.VMEM)
    dma = pltpu.SemaphoreType.DMA
    arrays = (
        tokens, mix_gain.reshape(1, -1), wq, wk, wv, wcv, wcg, query_gain.reshape(1, -1), key_gain.reshape(1, -1),
        sinks.reshape(1, -1), taps, conv_gain.reshape(1, -1), attn_proj.T, conv_proj.T,
    )
    return pl.pallas_call(
        kernel,
        out_shape=jax.ShapeDtypeStruct((256, 2048), BF),
        in_specs=[pl.BlockSpec(memory_space=pltpu.HBM)] * 14,
        out_specs=vmem,
        scratch_shapes=[
            *(pltpu.VMEM(a.shape, a.dtype) for a in arrays[1:]),
            pltpu.VMEM((2, 4, 4, 128, 896), BF),
            pltpu.VMEM((2, 4, 4, 512, 128), BF),
            pltpu.VMEM((64, 896), BF),
            pltpu.VMEM((128, 256), BF),
            pltpu.VMEM((128, 256), BF),
            pltpu.VMEM((2, 40, 256), F32),
            pltpu.VMEM((2, 128, 512), BF),
            pltpu.VMEM((2, 2, 4, 16, 128), BF),
            pltpu.VMEM((2, 2, 4, 16, 128), BF),
            pltpu.VMEM((2, 4, 256, 512), BF),
            pltpu.VMEM((512, 2048), BF),
            pltpu.VMEM((4, 512, 128), BF),
            pltpu.VMEM((2, 2, 512, 128), BF),
            pltpu.VMEM((2, 4, 288, 128), F32),
            pltpu.VMEM((4, 512, 128), F32),
            pltpu.VMEM((512, 128), F32),
            pltpu.VMEM((512, 128), F32),
            pltpu.VMEM((512, 1024), BF),
            pltpu.VMEM((4, 2, 256, 512), F32),
            pltpu.VMEM((4, 2, 256, 512), BF),
            pltpu.VMEM((4, 256, 512), BF),
            dma((13,)), dma((POOL,)), dma((SLOT_COUNT,)), dma((2,)), dma((4,)), dma((2,)), dma((4,)), dma(()), dma((2,)),
            dma((8,)), dma((1,)), dma((4,)),
        ],
        compiler_params=pltpu.CompilerParams(
            collective_id=0, has_side_effects=True, vmem_limit_bytes=44 * 1024 * 1024
        ),
        name="layer",
    )(*(pltpu.with_memory_space_constraint(a, pltpu.HBM) for a in arrays))


def solution(mesh):
    placed = (
        P("sp", "tp"), P(), P("sp", "tp"), P("sp", "tp"), P("sp", "tp"), P("sp", "tp"), P("sp", "tp"),
        P(), P(), P("tp"), P(None, "tp"), P("tp"), P("tp", "sp"), P("tp", "sp"),
    )
    return jax.shard_map(
        on_device, mesh=mesh, in_specs=placed, out_specs=P(("sp", "tp"), None), check_vma=False
    )
```

```python
import jax
import jax.numpy as jnp
from jax import lax
from jax.experimental import pallas as pl
from jax.experimental.pallas import tpu as pltpu
from jax.sharding import PartitionSpec as P

MESH = pl.DeviceIdType.MESH
EPSILON = 0.1
BF = jnp.bfloat16
F32 = jnp.float32

CV, CG, Q, KV = (0, 256), (256, 512), (512, 768), (768, 896)
STAGES = (
    ("w", 0, 512, ((0, 64, 32), (64, 16, 16), (80, 48, 32))),
    ("w", 512, 384, ((0, 48, 32), (48, 16, 16), (64, 64, 32))),
    ("p", 0, 128, ((0, 160, 80), (160, 192, 96), (352, 160, 80))),
)
ORDERS = ("xyz", "yzx", "zxy")
SLOTS = {(False, True): range(2), (False, False): range(3), (True, True): range(4), (True, False): range(6)}
SLOT_COUNT = 3 * sum(
    len(SLOTS[phase > 0, axis == "x"]) for order in ORDERS for phase, axis in enumerate(order)
)
POOL = 112


def kernel(
    tokens, *rest,
):
    given, (out, *held), rest = rest[:13], rest[13:27], rest[27:]
    mix_gain, wq, wk, wv, wcv, wcg, query_gain, key_gain, sinks, taps, conv_gain, attn_proj, conv_proj = held
    (
        w, p, mine_w, mine_p, peer_p, small, hop, edge_send, edge_recv, x_buf, normed, qn, kve, ge, conv, stat_own,
        stat_peer, feats, part_own, part_send, part_recv,
        load_sem, pool, ag_recv, d2d_recv, tok_recv, hop_recv, fwd_recv, loc_sem, sm_recv, halo_recv, stat_recv,
        out_recv,
    ) = rest
    loads = [pltpu.make_async_copy(a, b, load_sem.at[i]) for i, (a, b) in enumerate(zip(given, held))]
    for load in loads:
        load.start()
    sp, x = lax.axis_index("sp"), lax.axis_index("tp")
    k = lax.rem(sp, 2)
    q = sp // 2
    y, z = lax.rem(q, 4), q // 4
    pos = lax.rem(x + 4 - 2 * k, 4)
    xi0 = lax.rem(x, 2)
    is_source = pos < 2
    bufs = {"w": w, "p": p}

    def dev(xx, yy, zz, kk):
        return (zz * 8 + yy * 2 + kk, xx)

    def up(v, n=1):
        return lax.rem(v + n, 4)

    peer = dev(x, y, z, 1 - k)
    sends = []

    def copy(src, dst, ssem, rsem, device):
        return pltpu.make_async_remote_copy(
            src_ref=src, dst_ref=dst, send_sem=ssem, recv_sem=rsem, device_id=device, device_id_type=MESH
        )

    free = list(range(POOL))

    def send(src, dst, rsem, device, cond=None):
        ssem = free.pop(0)

        def go():
            copy(src, dst, pool.at[ssem], rsem, device).start()

        if cond is None:
            go()
        else:
            pl.when(cond)(go)
        sends.append((src, dst, ssem, rsem, device, cond))

    def recv(dst, rsem, cond=None):
        def go():
            copy(dst, dst, pool.at[0], rsem, peer).wait_recv()

        if cond is None:
            go()
        else:
            pl.when(cond)(go)

    def ref_of(stage, color, phase, where, half):
        name, c0, cn, rows = STAGES[stage]
        buf = bufs[name]
        r0, rn, rh = rows[color]
        cols = pl.ds(c0, cn)
        rr = pl.ds(r0, rn)
        two = {None: slice(None), 0: pl.ds(0, 2), 1: pl.ds(2, 2)}
        one = {None: slice(None), 0: pl.ds(0, 1), 1: pl.ds(1, 1)}
        axis = ORDERS[color][phase]
        if phase == 0:
            if axis == "x":
                return buf.at[where, z, y, rr, cols]
            if axis == "y":
                return buf.at[xi0, z, where, rr, cols]
            return buf.at[xi0, where, y, rr, cols]
        if color == 0:
            if axis == "y":
                return buf.at[one[half], z, where, rr, cols]
            return buf.at[one[half], where, :, rr, cols]
        if color == 1:
            if axis == "z":
                return buf.at[xi0, where, two[half], rr, cols]
            return buf.at[where, two[half], :, rr, cols]
        if axis == "x":
            return buf.at[where, two[half], y, rr, cols]
        return buf.at[one[half], :, where, rr, cols]

    slots = {}

    def first_slot(stage, color):
        return slots[stage, color, 0, 0]

    def context(stage, color, phase):
        axis = ORDERS[color][phase]
        rs = [ag_recv.at[slots.setdefault((stage, color, phase, i), len(slots))] for i in SLOTS[phase > 0, axis == "x"]]
        only_sources = is_source if ORDERS[color].index("x") > phase else None
        return axis, rs, only_sources

    def ring(axis):
        if axis == "y":
            return y, dev(x, up(y), z, k), dev(x, up(y, 3), z, k)
        return z, dev(x, y, up(z), k), dev(x, y, up(z, 3), k)

    def start1(stage, color, phase):
        axis, rs, cond = context(stage, color, phase)
        if axis == "x":
            if phase == 0:
                r = ref_of(stage, color, phase, xi0, None)
                for d in (1, 3, 2):
                    send(r, r, ag_recv.at[first_slot(stage, color) + xi0], dev(up(x, d), y, z, k), is_source)
                return
            inward = dev(jnp.where(pos == 0, up(x), up(x, 3)), y, z, k)
            outward = dev(jnp.where(pos == 0, up(x, 3), up(x)), y, z, k)
            h0, h1 = (ref_of(stage, color, phase, xi0, h) for h in (0, 1))
            send(h0, h0, rs[0], inward, is_source)
            send(h1, h1, rs[0], outward, is_source)
            send(h1, h1, rs[1], inward, is_source)
            send(h0, h0, rs[1], outward, is_source)
        else:
            at, right, left = ring(axis)
            if phase == 0:
                r = ref_of(stage, color, phase, at, None)
                send(r, r, rs[0], right, cond)
                send(r, r, rs[1], left, cond)
                across = dev(x, up(y, 2), z, k) if axis == "y" else dev(x, y, up(z, 2), k)
                send(r, r, rs[2], across, cond)
                return
            h0, h1 = (ref_of(stage, color, phase, at, h) for h in (0, 1))
            send(h0, h0, rs[0], right, cond)
            send(h1, h1, rs[1], left, cond)
            send(h1, h1, rs[2], right, cond)
            send(h0, h0, rs[3], left, cond)

    def turn(stage, color, phase):
        axis, rs, cond = context(stage, color, phase)
        if axis == "x":
            other = 1 - xi0
            h0, h1 = (ref_of(stage, color, phase, other, h) for h in (0, 1))
            to_low = dev(jnp.where(pos == 0, up(x, 3), up(x)), y, z, k)
            to_high = dev(jnp.where(pos == 2, up(x), up(x, 3)), y, z, k)
            recv(h0, rs[0], pos < 2)
            recv(h1, rs[0], pos >= 2)
            send(h0, h0, rs[2], to_low, pos < 2)
            send(h1, h1, rs[3], to_high, pos >= 2)
        else:
            at, right, left = ring(axis)
            h0 = ref_of(stage, color, phase, up(at, 3), 0)
            h1 = ref_of(stage, color, phase, up(at), 1)
            recv(h0, rs[0], cond)
            send(h0, h0, rs[4], right, cond)
            recv(h1, rs[1], cond)
            send(h1, h1, rs[5], left, cond)

    def finish(stage, color, phase):
        axis, rs, cond = context(stage, color, phase)
        if axis == "x":
            other = 1 - xi0
            if phase == 0:
                base = first_slot(stage, color)
                recv(ref_of(stage, color, phase, other, None), ag_recv.at[base + other])
                recv(ref_of(stage, color, phase, xi0, None), ag_recv.at[base + xi0], pos >= 2)
                return
            recv(ref_of(stage, color, phase, other, 1), rs[1], pos < 2)
            recv(ref_of(stage, color, phase, other, 0), rs[1], pos >= 2)
            recv(ref_of(stage, color, phase, xi0, 0), rs[2], pos >= 2)
            recv(ref_of(stage, color, phase, xi0, 1), rs[3], pos >= 2)
        else:
            at, _, _ = ring(axis)
            if phase == 0:
                for d, i in ((3, 0), (1, 1), (2, 2)):
                    recv(ref_of(stage, color, phase, up(at, d), None), rs[i], cond)
                return
            recv(ref_of(stage, color, phase, up(at, 3), 1), rs[2], cond)
            recv(ref_of(stage, color, phase, up(at), 0), rs[3], cond)
            recv(ref_of(stage, color, phase, up(at, 2), 0), rs[4], cond)
            recv(ref_of(stage, color, phase, up(at, 2), 1), rs[5], cond)

    def all_colors(step, stage, phase):
        for color in range(3):
            step(stage, color, phase)

    def flush(count=None):
        for _ in range(len(sends) if count is None else count):
            src, dst, ssem, rsem, device, cond = sends.pop(0)

            def done():
                copy(src, dst, pool.at[ssem], rsem, device).wait_send()

            if cond is None:
                done()
            else:
                pl.when(cond)(done)
            free.append(ssem)

    own_rows = pl.ds(pl.multiple_of(k * 64, 64), 64)
    barrier = pltpu.get_barrier_semaphore()
    y_up, z_up = up(y), up(z)
    partners = [
        peer, dev(up(x), y, z, k), dev(up(x, 3), y, z, k),
        dev(x, y_up, z, k), dev(x, up(y, 3), z, k), dev(x, y, z_up, k), dev(x, y, up(z, 3), k),
        dev(up(x, 2), y, z, k), dev(x, up(y, 2), z, k), dev(x, y, up(z, 2), k),
    ]
    for partner in partners:
        pl.semaphore_signal(barrier, inc=1, device_id=partner, device_id_type=MESH)
    own = pl.multiple_of(x * 256, 256)
    local = pltpu.make_async_copy(tokens.at[pl.ds(own, 256), :], x_buf.at[k, x], loc_sem)
    local.start()
    for load in loads:
        load.wait()
    shard = jnp.concatenate([wcv[...], wcg[...], wq[...], wk[...], wv[...]], axis=1)

    @pl.when(is_source)
    def _():
        w[xi0, z, y, own_rows, :] = shard

    @pl.when(jnp.logical_not(is_source))
    def _():
        mine_w[...] = shard

    mine_p[...] = jnp.concatenate([attn_proj[...], conv_proj[...]], axis=0)
    small[xi0, 0:31, :] = taps[...]
    small[xi0, 31:32, :] = conv_gain[...]
    small[xi0, 32:33, :] = jnp.concatenate(
        [jnp.broadcast_to(sinks[:, h : h + 1], (1, 64)) for h in range(4)], axis=1
    )

    pl.semaphore_wait(barrier, len(partners))

    not_source = jnp.logical_not(is_source)
    slot = w.at[xi0, z, y, own_rows, :]
    send(mine_w, slot, d2d_recv.at[0], peer, not_source)
    send(mine_p, peer_p, d2d_recv.at[1], peer)
    peer_rows = pl.ds(pl.multiple_of((1 - k) * 64, 64), 64)
    recv(w.at[xi0, z, y, peer_rows, :], d2d_recv.at[0], is_source)
    all_colors(start1, 0, 0)
    all_colors(start1, 1, 0)

    right, left, across = dev(up(x), y, z, k), dev(up(x, 3), y, z, k), up(x, 2)

    def token_sends(far):
        for to, device, i in ((up(x), right, 0), (up(x, 3), left, 1)):
            if far:
                block = tokens.at[pl.ds(pl.multiple_of(across * 256 + i * 128, 128), 128), :]
                send(block, hop.at[i], hop_recv.at[i], device)
            else:
                block = tokens.at[pl.ds(pl.multiple_of(to * 256, 256), 256), :]
                send(block, x_buf.at[k, x], tok_recv.at[i], device)

    def token_hops():
        for origin, device, i in ((up(x, 3), right, 0), (up(x), left, 1)):
            recv(hop.at[i], hop_recv.at[i])
            send(hop.at[i], x_buf.at[k, origin, pl.ds(i * 128, 128), :], tok_recv.at[2 + i], device)

    def tokens_near():
        for i, origin in ((0, up(x, 3)), (1, up(x))):
            recv(x_buf.at[k, origin], tok_recv.at[i])
            send(x_buf.at[k, origin], x_buf.at[k, origin], fwd_recv.at[1 + i], peer)

    def tokens_far():
        for i in (0, 1):
            recv(x_buf.at[k, across, pl.ds(i * 128, 128), :], tok_recv.at[2 + i])
        send(x_buf.at[k, across], x_buf.at[k, across], fwd_recv.at[3], peer)

    def small_on():
        recv(small.at[1 - xi0], sm_recv.at[1 - xi0])
        beyond = dev(jnp.where(jnp.logical_or(pos == 0, pos == 3), up(x, 3), up(x)), y, z, k)
        send(small.at[1 - xi0], small.at[1 - xi0], sm_recv.at[1 - xi0], beyond, is_source)

    recv(peer_p, d2d_recv.at[1])

    @pl.when(is_source)
    def _():
        a, b = mine_p[...], peer_p[...]
        low = jnp.where(k == 0, a, b)
        high = jnp.where(k == 0, b, a)
        p[xi0, z, y, 0:256, :] = jnp.concatenate([low[:64], high[:64]], axis=0).T
        p[xi0, z, y, 256:512, :] = jnp.concatenate([low[64:], high[64:]], axis=0).T

    def onward(last, following):
        for color in range(3):
            finish(last[0], color, last[1])
            start1(following[0], color, following[1])

    all_colors(start1, 2, 0)
    onward((0, 0), (0, 1))
    onward((1, 0), (1, 1))
    token_sends(True)
    all_colors(finish, 2, 0)
    initial = len(sends)
    all_colors(turn, 0, 1)
    all_colors(start1, 2, 1)
    all_colors(turn, 1, 1)
    token_sends(False)
    send(tokens.at[pl.ds(own, 256), :], x_buf.at[k, x], fwd_recv.at[0], peer)
    mine_small = small.at[xi0]
    for device in (right, left):
        send(mine_small, mine_small, sm_recv.at[xi0], device, is_source)
    onward((0, 1), (0, 2))
    early = len(sends) - initial
    token_hops()
    flush(initial)
    all_colors(turn, 2, 1)
    for color in (0, 2, 1):
        turn(0, color, 2)
        finish(1, color, 1)
        start1(1, color, 2)
        if color == 2:
            tokens_near()
    tokens_far()
    small_on()
    local.wait()

    def norm_rows(s):
        def body(r, _):
            rows = pl.ds(pl.multiple_of(r * 32, 32), 32)
            parts = [x_buf[s, f, rows, :].astype(F32) for f in range(4)]
            square = sum(jnp.sum(v * v, axis=-1, keepdims=True) for v in parts)
            scale = lax.rsqrt(square * (1.0 / 2048) + EPSILON)
            for f in range(4):
                normed[pl.ds(pl.multiple_of(s * 256 + r * 32, 32), 32), f * 512 : f * 512 + 512] = (
                    parts[f] * scale * mix_gain[:, f * 512 : f * 512 + 512]
                ).astype(BF)
            return 0

        lax.fori_loop(0, 8, body, 0)

    norm_rows(k)
    recv(x_buf.at[1 - k, x], fwd_recv.at[0])
    for i, origin in ((1, up(x, 3)), (2, up(x)), (3, across)):
        recv(x_buf.at[1 - k, origin], fwd_recv.at[i])
    norm_rows(1 - k)
    flush(early)
    middle = len(sends)
    all_colors(finish, 2, 1)
    all_colors(finish, 0, 2)

    lane = lax.broadcasted_iota(jnp.int32, (256, 128), 1)
    low_lane = lane < 64
    key_row = jnp.concatenate([key_gain[...], jnp.ones_like(key_gain[...])], axis=1)
    query_row = jnp.concatenate([query_gain[...], query_gain[...]], axis=1)

    def project(s, xi, cols):
        lhs = normed[pl.ds(s * 256, 256), :]
        rhs = w[xi, :, :, :, cols[0] : cols[1]].reshape(2048, cols[1] - cols[0])
        return jnp.dot(lhs, rhs, preferred_element_type=F32)

    def gated_part(s, xi):
        both = project(s, xi, (0, 512))
        value, gate = both[:, :256], both[:, 256:]
        rounded = (value * jax.nn.sigmoid(gate)).astype(BF)
        gated = rounded.astype(F32)
        for half in (0, 1):
            lanes = slice(half * 128, half * 128 + 128)
            ge[s, xi * 2 + half, 16:272, :] = gated[:, lanes]
            edge_send[s, 0, xi * 2 + half] = rounded[240:, lanes]
            edge_send[s, 1, xi * 2 + half] = rounded[:16, lanes]

    def neighbour(s, side):
        wraps, over = (x == 3, 1) if side == 0 else (x == 0, 15)
        step = jnp.where(jnp.logical_and(wraps, s == 1 - side), over, 0)
        return (lax.rem(q + step, 16) * 2 + k, up(x, 1 if side == 0 else 3)), jnp.where(wraps, 1 - s, s)

    SIDES = ((0, 0), (0, 1), (1, 0), (1, 1))
    is_first = jnp.logical_and(q == 0, x == 0)
    is_last = jnp.logical_and(q == 15, x == 3)

    for s in (0, 1):
        for xi in (0, 1):
            gated_part(s, xi)
        for side in (0, 1):
            to, seg = neighbour(s, side)
            send(edge_send.at[s, side], edge_recv.at[seg, side], halo_recv.at[4 + seg * 2 + side], to)
    all_colors(turn, 1, 2)
    all_colors(start1, 2, 2)
    recv(small.at[xi0], sm_recv.at[xi0], not_source)
    def conv_block(segment, cb, chunks):
        xi, half = cb // 2, lax.rem(cb, 2)
        tap_rows = jnp.where(half == 0, small[xi, :, 0:128], small[xi, :, 128:256])
        for r, n in chunks:
            total = jnp.zeros((n, 128), F32)
            for t in range(31):
                total = total + tap_rows[t : t + 1, :] * ge[segment, cb, r + 1 + t : r + 1 + n + t, :]
            conv[cb, segment * 256 + r : segment * 256 + r + n, :] = total

    for s in (0, 1):
        def inner_step(cb, _, s=s):
            conv_block(s, cb, ((16, 112), (128, 112)))
            return 0

        lax.fori_loop(0, 4, inner_step, 0)
    for s in (0, 1):
        for side in (0, 1):
            recv(edge_recv.at[s, side], halo_recv.at[4 + s * 2 + side])
            ge[s, :, side * 272 : side * 272 + 16, :] = edge_recv[s, side].astype(F32)

        @pl.when(is_first if s == 0 else is_last)
        def _():
            ge[s, :, s * 272 : s * 272 + 16, :] = jnp.zeros((4, 16, 128), F32)

        def outer_step(cb, _, s=s):
            conv_block(s, cb, ((0, 16), (240, 16)))
            return 0

        lax.fori_loop(0, 4, outer_step, 0)
    def stats(i, _):
        rows = pl.ds(pl.multiple_of(i * 64, 64), 64)
        blocks = [conv[cb, rows, :] for cb in range(4)]
        mean = jnp.sum(blocks[0] + blocks[1] + blocks[2] + blocks[3], axis=-1, keepdims=True) * (1.0 / 512)
        dev_sq = sum((b - mean) * (b - mean) for b in blocks)
        m2 = jnp.sum(dev_sq, axis=-1, keepdims=True)
        stat_own[rows, :] = jnp.where(low_lane[:64], mean, m2)
        return 0

    lax.fori_loop(0, 8, stats, 0)
    send(stat_own, stat_peer, stat_recv.at[0], peer)

    all_colors(finish, 1, 2)

    def project_both(s, cols):
        lhs = normed[pl.ds(s * 256, 256), :]
        width = cols[1] - cols[0]
        rhs = jnp.concatenate([w[xi, :, :, :, cols[0] : cols[1]].reshape(2048, width) for xi in (0, 1)], axis=1)
        both = jnp.dot(lhs, rhs, preferred_element_type=F32)
        return both[:, :width], both[:, width:]

    def first_part(s, _):
        for xi, kv in enumerate(project_both(s, KV)):
            square = jnp.sum(jnp.where(low_lane, kv * kv, 0.0), axis=-1, keepdims=True)
            keyed = kv * lax.rsqrt(square * (1.0 / 64) + EPSILON) * key_row
            kve[s, xi, 128:384, :] = jnp.where(low_lane, keyed, kv).astype(BF)
        return 0

    for s, side in SIDES:
        if side == 0:
            first_part(s, 0)
        to, seg = neighbour(s, side)
        src, dst = (256, 0) if side == 0 else (128, 384)
        send(kve.at[s, :, pl.ds(src, 128), :], kve.at[seg, :, pl.ds(dst, 128), :], halo_recv.at[seg * 2 + side], to)
    def query_part(s, _):
        for xi, full in enumerate(project_both(s, Q)):
            for pair in (0, 1):
                v = full[:, pair * 128 : pair * 128 + 128]
                sq = v * v
                even = jnp.sum(jnp.where(low_lane, sq, 0.0), axis=-1, keepdims=True)
                odd = jnp.sum(jnp.where(low_lane, 0.0, sq), axis=-1, keepdims=True)
                scale = lax.rsqrt(jnp.where(low_lane, even, odd) * (1.0 / 64) + EPSILON)
                rounded = (v * scale * query_row).astype(BF).astype(F32) * 0.125
                qn[xi * 2 + pair, pl.ds(s * 256, 256), :] = rounded.astype(BF)
        return 0

    for s in (0, 1):
        query_part(s, 0)
    late = len(sends) - middle
    for color in (0, 2, 1):
        turn(2, color, 2)
    recv(stat_peer, stat_recv.at[0])

    def feature(i, _):
        rows = pl.ds(pl.multiple_of(i * 64, 64), 64)
        a, b = stat_own[rows, :], stat_peer[rows, :]
        mean = 0.5 * (a[:, 0:1] + b[:, 0:1])
        gap = a[:, 0:1] - b[:, 0:1]
        spread = (a[:, 64:65] + b[:, 64:65] + gap * gap * 256.0) * (1.0 / 1024)
        scale = lax.rsqrt(spread + EPSILON)
        for cb in range(4):
            xi, half = cb // 2, cb % 2
            gain = small[xi, 31:32, half * 128 : half * 128 + 128]
            v = (conv[cb, rows, :] - mean) * scale * gain
            feats[rows, xi * 512 + 256 + half * 128 : xi * 512 + 384 + half * 128] = (v * jax.nn.sigmoid(v)).astype(BF)
        return 0

    lax.fori_loop(0, 8, feature, 0)
    flush(middle)
    row_i = lax.rem(lax.broadcasted_iota(jnp.int32, (256, 384), 0), 128)
    col_i = lax.broadcasted_iota(jnp.int32, (256, 384), 1)
    lane384 = lax.broadcasted_iota(jnp.int32, (384, 128), 1) < 64

    def attention(i):
        s, b = i // 2, i % 2
        base = s * 256 + b * 128
        first = jnp.where(jnp.logical_and(is_first, s == 0), 128, 0) - b * 128
        end = jnp.where(jnp.logical_and(is_last, s == 1), 384, 512) - b * 128
        reach = col_i - row_i
        allowed = (reach >= 0) & (reach <= 256) & (col_i >= first) & (col_i < end)
        nt = (((1,), (1,)), ((), ()))

        def mix(heads, keys, values):
            scores = lax.dot_general(heads, keys.astype(BF), nt, preferred_element_type=F32)
            weights = jnp.where(allowed, jnp.exp(scores), 0.0).astype(BF)
            return jnp.dot(weights, values.astype(BF), preferred_element_type=F32)

        for xi in (0, 1):
            kv = kve[s, xi, b * 128 : b * 128 + 384, :].astype(F32)
            swapped = pltpu.roll(kv, 64, 1)
            both = jnp.concatenate([qn[xi * 2 + pair, pl.ds(base, 128), :] for pair in (0, 1)], axis=0).astype(F32)
            even = jnp.where(low_lane, both, 0.0).astype(BF)
            odd = jnp.where(low_lane, 0.0, both).astype(BF)
            o_even = mix(even, kv, jnp.where(lane384, swapped, 1.0))
            o_odd = mix(odd, swapped, jnp.where(lane384, 1.0, kv))
            number = jnp.where(low_lane, o_even, o_odd)
            weight = pltpu.roll(jnp.where(low_lane, o_odd, o_even), 64, 1)
            sink = jnp.exp(small[xi, 32:33, :])
            for pair in (0, 1):
                rows, lanes = slice(pair * 128, pair * 128 + 128), slice(pair * 128, pair * 128 + 128)
                col = xi * 512 + pair * 128
                feats[pl.ds(base, 128), col : col + 128] = (number[rows] / (weight[rows] + sink[:, lanes])).astype(BF)

    for s, b in SIDES:
        recv(kve.at[s, :, pl.ds(b * 384, 128), :], halo_recv.at[s * 2 + b])
        attention(s * 2 + b)

    flush(late)
    all_colors(finish, 2, 2)

    for nb in range(4):
        rhs = jnp.concatenate(
            [jnp.concatenate([p[xi, nb, yy] for yy in range(4)], axis=1) for xi in (0, 1)], axis=0
        )
        part = jnp.dot(feats[...], rhs, preferred_element_type=F32).reshape(2, 256, 512)
        part_send[nb] = part.astype(BF)
        send(part_send.at[nb, 1 - k], part_recv.at[nb], out_recv.at[nb], peer)
        part_own[nb] = part
    for nb in range(4):
        recv(part_recv.at[nb], out_recv.at[nb])
        out[:, nb * 512 : nb * 512 + 512] = (part_own[nb, k] + part_recv[nb].astype(F32)).astype(BF)
    flush()


def on_device(tokens, mix_gain, wq, wk, wv, wcv, wcg, query_gain, key_gain, sinks, taps, conv_gain, attn_proj, conv_proj):
    vmem = pl.BlockSpec(memory_space=pltpu.VMEM)
    dma = pltpu.SemaphoreType.DMA
    arrays = (
        tokens, mix_gain.reshape(1, -1), wq, wk, wv, wcv, wcg, query_gain.reshape(1, -1), key_gain.reshape(1, -1),
        sinks.reshape(1, -1), taps, conv_gain.reshape(1, -1), attn_proj.T, conv_proj.T,
    )
    return pl.pallas_call(
        kernel,
        out_shape=jax.ShapeDtypeStruct((256, 2048), BF),
        in_specs=[pl.BlockSpec(memory_space=pltpu.HBM)] * 14,
        out_specs=vmem,
        scratch_shapes=[
            *(pltpu.VMEM(a.shape, a.dtype) for a in arrays[1:]),
            pltpu.VMEM((2, 4, 4, 128, 896), BF),
            pltpu.VMEM((2, 4, 4, 512, 128), BF),
            pltpu.VMEM((64, 896), BF),
            pltpu.VMEM((128, 256), BF),
            pltpu.VMEM((128, 256), BF),
            pltpu.VMEM((2, 40, 256), F32),
            pltpu.VMEM((2, 128, 512), BF),
            pltpu.VMEM((2, 2, 4, 16, 128), BF),
            pltpu.VMEM((2, 2, 4, 16, 128), BF),
            pltpu.VMEM((2, 4, 256, 512), BF),
            pltpu.VMEM((512, 2048), BF),
            pltpu.VMEM((4, 512, 128), BF),
            pltpu.VMEM((2, 2, 512, 128), BF),
            pltpu.VMEM((2, 4, 288, 128), F32),
            pltpu.VMEM((4, 512, 128), F32),
            pltpu.VMEM((512, 128), F32),
            pltpu.VMEM((512, 128), F32),
            pltpu.VMEM((512, 1024), BF),
            pltpu.VMEM((4, 2, 256, 512), F32),
            pltpu.VMEM((4, 2, 256, 512), BF),
            pltpu.VMEM((4, 256, 512), BF),
            dma((13,)), dma((POOL,)), dma((SLOT_COUNT,)), dma((2,)), dma((4,)), dma((2,)), dma((4,)), dma(()), dma((2,)),
            dma((8,)), dma((1,)), dma((4,)),
        ],
        compiler_params=pltpu.CompilerParams(
            collective_id=0, has_side_effects=True, vmem_limit_bytes=44 * 1024 * 1024
        ),
        name="layer",
    )(*(pltpu.with_memory_space_constraint(a, pltpu.HBM) for a in arrays))


def solution(mesh):
    placed = (
        P("sp", "tp"), P(), P("sp", "tp"), P("sp", "tp"), P("sp", "tp"), P("sp", "tp"), P("sp", "tp"),
        P(), P(), P("tp"), P(None, "tp"), P("tp"), P("tp", "sp"), P("tp", "sp"),
    )
    return jax.shard_map(
        on_device, mesh=mesh, in_specs=placed, out_specs=P(("sp", "tp"), None), check_vma=False
    )
```
